32 devices in a mesh: sp: 8 (over z, x), tp: 4 (over y, core).
Axes of the slice: x: 2, y: 2, z: 4, core: 2. Of those that a mesh axis runs over, the one named last changes fastest.
Arguments:
- inputs: bfloat16 [5120, 2048], P('sp', 'tp'), may hold values from -6 to 6
- norm_gain: bfloat16 [2048], P('tp'), may hold values from 0.099609375 to 1.8984375
- query_weight: bfloat16 [2048, 2048], P('sp', 'tp'), may hold values from -0.125 to 0.125
- key_weight: bfloat16 [2048, 2048], P('sp', 'tp'), may hold values from -0.125 to 0.125
- value_weight: bfloat16 [2048, 2048], P('sp', 'tp'), may hold values from -0.125 to 0.125
- outgate_weight: bfloat16 [2048, 2048], P('sp', 'tp'), may hold values from -0.125 to 0.125
- inputgate_weight: bfloat16 [2048, 8], replicated, may hold values from -1 to 1
- forget_weight: bfloat16 [2048, 8], replicated, may hold values from -0.125 to 0.125
- forget_bias: float32 [8], P('tp'), may hold values from -1.1 to 2.25
- conv_query: float32 [4, 2048], P(None, 'tp'), may hold values from -3 to 3
- conv_key: float32 [4, 2048], P(None, 'tp'), may hold values from -3 to 3
- cell_gain: float32 [2048], P('tp'), may hold values from 0.1 to 1.9
- pool_weight: bfloat16 [2048, 1024], P('sp', 'tp'), may hold values from -0.125 to 0.125
- group_weight: bfloat16 [8, 128, 128], P('tp'), may hold values from -0.5 to 0.5
- pool_gain: float32 [1024], P('tp'), may hold values from 0.1 to 1.9
- cell_out_weight: bfloat16 [2048, 2048], P('tp', 'sp'), may hold values from -0.109375 to 0.109375
- pool_out_weight: bfloat16 [1024, 2048], P('tp', 'sp'), may hold values from -0.109375 to 0.109375
Outputs:
- mixed: bfloat16 [5120, 2048], P(('sp', 'tp'))
The draws below stay inside these ranges and needn't reach their ends.
All inputs are finite; a program needn't handle non-finite values.
Results may differ from the reference program's by a relative error of at most 0.013.
The reference program's roundings to bfloat16 on the way (of `normed`, `cell_mix`, `pooled` and `pool_mix`) count: a program that leaves them out, or rounds other values in their place, can miss the bound.
Values may be sent and summed in bfloat16 or wider, within the bound.
A program may use at most 128 MiB of HBM per device.

```python
import math
import jax
import jax.numpy as jnp
from jax import lax

D = 2048
HM = 8
DH = 256
PG = 8
CG = 128
LEVELS = 4
CONV = 4
TOK_DEV = 640
TOKENS = 5120
N_SP = 8


def draw_inputs(key, part):
    jitter = jax.random.normal(jax.random.fold_in(key, 12), (TOKENS, D), jnp.float32)
    values = jnp.clip(jitter, -6.0, 6.0)
    return values.astype(jnp.bfloat16)


def draw_inputgate_weight(key, part):
    spread = D ** (-0.5)
    jitter = jnp.clip(jax.random.normal(jax.random.fold_in(key, 13), (D, HM), jnp.float32), -6.0, 6.0) * spread
    values = jitter
    return values.astype(jnp.bfloat16)


def block_scale(own_key, shape, cuts, smallest, top_value):
    def one(dim, blocks):
        draws = jax.random.uniform(jax.random.fold_in(jax.random.fold_in(own_key, 6), dim), (blocks,), jnp.float32, smallest / len(cuts), top_value / len(cuts))
        return jnp.repeat(jnp.exp(draws), shape[dim] // blocks).reshape((-1,) + (1,) * (len(shape) - dim - 1))

    gain = one(*cuts[0])
    for cut in cuts[1:]:
        gain = gain * one(*cut)
    return gain


def normal_values(key, extent, width, most, split=(), kind=jnp.bfloat16):
    values = jax.random.normal(key, extent, jnp.float32) * width
    if len(split) > 0:
        values = block_scale(key, extent, split, -0.22, 0.18) * values
    return jnp.clip(values, min=-most, max=most).astype(kind)


def setup_inputs(seed: int = 0) -> dict:
    key_of = jax.random.split(jax.random.key(seed), 18)
    return {
        "inputs": draw_inputs(jax.random.fold_in(key_of[17], 71), 0),
        "norm_gain": jnp.clip(1.0 + 0.18 * jax.random.normal(key_of[1], (D,), jnp.float32), 0.099609375, 1.8984375).astype(jnp.bfloat16),
        "query_weight": normal_values(key_of[2], (D, HM * DH), D ** -0.5, 0.125, ((0, 8), (1, 4))),
        "key_weight": normal_values(key_of[3], (D, HM * DH), D ** -0.5, 0.125, ((0, 8), (1, 4))),
        "value_weight": normal_values(key_of[4], (D, HM * DH), D ** -0.5, 0.125, ((0, 8), (1, 4))),
        "outgate_weight": normal_values(key_of[5], (D, HM * DH), D ** -0.5, 0.125, ((0, 8), (1, 4))),
        "inputgate_weight": draw_inputgate_weight(jax.random.fold_in(key_of[17], 71), 0),
        "forget_weight": normal_values(key_of[7], (D, HM), D ** -0.5, 0.125),
        "forget_bias": jnp.clip(-1.1 + 3.35 * jax.random.uniform(key_of[8], (HM,), jnp.float32) ** block_scale(key_of[8], (HM,), ((0, 4),), -0.2, 0.2), -1.1, 2.25),
        "conv_query": normal_values(key_of[9], (CONV, HM * DH), CONV ** -0.5, 3.0, ((1, 4),), jnp.float32),
        "conv_key": normal_values(key_of[10], (CONV, HM * DH), CONV ** -0.5, 3.0, ((1, 4),), jnp.float32),
        "cell_gain": jnp.clip(1.0 + 0.18 * jax.random.normal(key_of[11], (HM * DH,), jnp.float32), 0.1, 1.9),
        "pool_weight": normal_values(key_of[12], (D, PG * CG), D ** -0.5, 0.125, ((0, 8), (1, 4))),
        "group_weight": normal_values(key_of[13], (PG, CG, CG), CG ** -0.5, 0.5, ((0, 4),)),
        "pool_gain": jnp.clip(1.0 + 0.18 * jax.random.normal(key_of[14], (PG * CG,), jnp.float32), 0.1, 1.9),
        "cell_out_weight": normal_values(key_of[15], (HM * DH, D), (HM * DH + PG * CG) ** -0.5, 0.109375, ((0, 4), (1, 8))),
        "pool_out_weight": normal_values(key_of[16], (PG * CG, D), (HM * DH + PG * CG) ** -0.5, 0.109375, ((0, 4), (1, 8))),
    }


epsilon = 1e-06
big_negative = -1e+30
highest = lax.Precision.HIGHEST

def causal_taps(padded, taps):
    span_rows = padded.shape[0] - taps.shape[0] + 1
    running = jnp.zeros((span_rows, padded.shape[1]), jnp.float32)
    for lag_index in range(taps.shape[0]):
        running = running + taps[lag_index] * padded[lag_index:lag_index + span_rows].astype(jnp.float32)
    return running

def cell_block(carry, block_inputs):
    memory, normalizer, stabilizer = carry
    queries, key_rows, value_rows, log_in, log_keep = block_inputs
    query_wide = queries.astype(jnp.float32)
    key_wide = key_rows.astype(jnp.float32)
    value_wide = value_rows.astype(jnp.float32)
    length = queries.shape[0]
    cumulative = jnp.cumsum(log_keep, axis=0)
    cum_heads = cumulative.T
    in_heads = log_in.T
    causal = jnp.arange(length)[:, None] >= jnp.arange(length)[None, :]
    decay_log = cum_heads[:, :, None] - cum_heads[:, None, :] + in_heads[:, None, :]
    decay_log = jnp.where(causal[None, :, :], decay_log, -jnp.inf)
    carried_log = cum_heads + stabilizer[:, None]
    ceiling = jnp.maximum(carried_log, lax.optimization_barrier(jnp.max(decay_log, axis=2)))
    within = jnp.exp(decay_log - ceiling[:, :, None])
    carried = jnp.exp(carried_log - ceiling)
    raw_scores = jnp.einsum('thd,shd->hts', query_wide, key_wide, precision=highest)
    scores = (raw_scores * within).astype(jnp.bfloat16).astype(jnp.float32)
    numerator = carried.T[:, :, None] * jnp.einsum('hvk,thk->thv', memory, query_wide, precision=highest)
    numerator = numerator + jnp.einsum('hts,shv->thv', scores, value_wide, precision=highest)
    denominator = carried.T * jnp.einsum('hk,thk->th', normalizer, query_wide, precision=highest) + lax.optimization_barrier(jnp.sum(scores, axis=2)).T
    hidden = numerator / jnp.maximum(jnp.abs(denominator), jnp.exp(-ceiling.T))[:, :, None]
    final_log = cumulative[-1]
    lead_log = final_log[None, :] - cumulative + log_in
    new_stab = jnp.maximum(final_log + stabilizer, lax.optimization_barrier(jnp.max(lead_log, axis=0)))
    share_weight = jnp.exp(lead_log - new_stab[None, :])
    fade_factor = jnp.exp(final_log + stabilizer - new_stab)
    weighted = (value_wide * share_weight[:, :, None]).astype(jnp.bfloat16).astype(jnp.float32)
    memory = fade_factor[:, None, None] * memory + jnp.einsum('shv,shk->hvk', weighted, key_wide, precision=highest)
    normalizer = fade_factor[:, None] * normalizer + jnp.einsum('sh,shk->hk', share_weight, key_wide, precision=highest)
    return ((memory, normalizer, new_stab), hidden)

def reference(inputs, norm_gain, query_weight, key_weight, value_weight, outgate_weight, inputgate_weight, forget_weight, forget_bias, conv_query, conv_key, cell_gain, pool_weight, group_weight, pool_gain, cell_out_weight, pool_out_weight):
    wide_in = inputs.astype(jnp.float32)
    inverse_rms = lax.rsqrt(lax.optimization_barrier(jnp.mean(wide_in * wide_in, axis=1, keepdims=True)) + epsilon)
    normed = (wide_in * norm_gain.astype(jnp.float32)).astype(jnp.bfloat16)

    def project(weight):
        return jnp.dot(normed, weight, preferred_element_type=jnp.float32) * inverse_rms
    query_pre = project(query_weight).astype(jnp.bfloat16)
    key_pre = project(key_weight).astype(jnp.bfloat16)
    value_rows = project(value_weight).astype(jnp.bfloat16)
    outgate_pre = project(outgate_weight).astype(jnp.bfloat16)
    pool_pre = project(pool_weight).astype(jnp.bfloat16)
    log_in = project(inputgate_weight)
    log_keep = jax.nn.log_sigmoid(project(forget_weight) + forget_bias + math.log(TOKENS))
    margin = conv_query.shape[0] - 1
    query_taps = causal_taps(jnp.pad(query_pre, ((margin, 0), (0, 0))), conv_query)
    key_taps = causal_taps(jnp.pad(key_pre, ((margin, 0), (0, 0))), conv_key)
    queries = (jax.nn.silu(query_taps) * DH ** (-0.5)).astype(jnp.bfloat16)
    key_rows = jax.nn.silu(key_taps).astype(jnp.bfloat16)

    def to_blocks(array):
        return array.reshape((N_SP, TOK_DEV) + array.shape[1:])

    def split_heads(array):
        return array.reshape(TOKENS, HM, DH)
    start_carry = (jnp.zeros((HM, DH, DH), jnp.float32), jnp.zeros((HM, DH), jnp.float32), jnp.full((HM,), big_negative, jnp.float32))
    block_inputs = (to_blocks(split_heads(queries)), to_blocks(split_heads(key_rows)), to_blocks(split_heads(value_rows)), to_blocks(log_in), to_blocks(log_keep))
    ignored, hidden = lax.scan(cell_block, start_carry, block_inputs)
    hidden = hidden.reshape(TOKENS, HM, DH)
    normalized = hidden * lax.rsqrt(lax.optimization_barrier(jnp.mean(hidden * hidden, axis=2, keepdims=True)) + epsilon)
    cell_mix = (normalized.reshape(TOKENS, HM * DH) * cell_gain * jax.nn.sigmoid(outgate_pre.astype(jnp.float32))).astype(jnp.bfloat16)
    widest = 2 ** LEVELS - 1
    padded_pool = jnp.pad(pool_pre, ((widest, 0), (0, 0))).astype(jnp.float32)
    position = jnp.arange(TOKENS)
    pieces = []
    for group_index in range(PG):
        reach_rows = 2 ** (1 + group_index % LEVELS)
        columns = padded_pool[:, group_index * CG:(group_index + 1) * CG]
        window_sum = jnp.zeros((TOKENS, CG), jnp.float32)
        for lag_index in range(reach_rows):
            window_sum = window_sum + columns[widest - lag_index:widest - lag_index + TOKENS]
        counted = jnp.minimum(position + 1, reach_rows).astype(jnp.float32)[:, None]
        pieces.append(window_sum / counted - columns[widest:])
    pooled = jnp.stack(pieces, axis=1).astype(jnp.bfloat16)
    grouped_out = jnp.einsum('sgc,gcd->sgd', pooled.astype(jnp.float32), group_weight.astype(jnp.float32), precision=highest)
    pool_mix = (grouped_out.reshape(TOKENS, PG * CG) * pool_gain).astype(jnp.bfloat16)
    mixed = jnp.dot(cell_mix, cell_out_weight, preferred_element_type=jnp.float32)
    mixed = mixed + jnp.dot(pool_mix, pool_out_weight, preferred_element_type=jnp.float32)
    return mixed.astype(jnp.bfloat16)
```

```python
import functools
import math

import jax
import jax.numpy as jnp
from jax import lax
from jax.experimental import pallas as pl
from jax.experimental.pallas import tpu as pltpu
from jax.sharding import PartitionSpec as P

LEVELS = 4

epsilon = 1e-06
big_negative = -1e30
highest = lax.Precision.HIGHEST
MESH = pl.DeviceIdType.MESH


def remote(src, dst, send, recv, device):
    return pltpu.make_async_remote_copy(
        src_ref=src, dst_ref=dst, send_sem=send, recv_sem=recv,
        device_id=device, device_id_type=MESH,
    )


def gather_kernel(
    pairs, tall, x_ref, wp_ref, wo_ref, x_out, wp_out, wo_out,
    local_sem, x_send, x_recv, s_send, s_recv, h_send, h_recv, r_send, r_recv,
):
    sp, tp = lax.axis_index("sp"), lax.axis_index("tp")
    pair, half = sp // 2, sp % 2
    row, side = tp // 2, tp % 2
    width = x_ref.shape[1]
    other = 2 * pair + 1 - half
    sibling = (sp, 2 * row + 1 - side)
    right = (2 * lax.rem(pair + 1, pairs) + half, tp)
    left = (2 * lax.rem(pair + pairs - 1, pairs) + half, tp)
    offsets = [(a, b) for a in range(2) for b in range(tall) if (a, b) != (0, 0)]
    group = [
        (2 * pair + lax.rem(half + a, 2), 2 * lax.rem(row + b, tall) + side) for a, b in offsets
    ]

    barrier = pltpu.get_barrier_semaphore()
    greeted = group + [sibling, right, left]
    for device in greeted:
        pl.semaphore_signal(barrier, inc=1, device_id=device, device_id_type=MESH)
    pl.semaphore_wait(barrier, len(greeted))

    def x_block(h, r, s):
        column = pl.multiple_of((2 * r + s) * width, width)
        return x_out.at[h, :, pl.ds(column, width)]

    def ring_copies(k, direction, item):
        if direction == 0:
            source = lax.rem(pair - k + 1 + pairs, pairs)
        else:
            source = lax.rem(pair + k - 1, pairs)
        place = 2 * source + (half if item == 0 else 1 - half)
        target = right if direction == 0 else left
        own = k == 1 and item == 0
        index = ((k - 1) * 2 + direction) * 2 + item
        out = []
        for j, (whole, mine) in enumerate(((wp_out, wp_ref), (wo_out, wo_ref))):
            src = mine.at[half] if own else whole.at[place]
            out.append(
                remote(src, whole.at[place], r_send.at[index, j], r_recv.at[index, j], target)
            )
        return out

    steps = pairs // 2

    def has(k, direction, item):
        return k < steps or (k == steps and direction == item)

    swap = [
        remote(wp_ref.at[1 - half], wp_out.at[sp], h_send.at[0], h_recv.at[0], (other, tp)),
        remote(wo_ref.at[1 - half], wo_out.at[sp], h_send.at[1], h_recv.at[1], (other, tp)),
    ]
    for copy in swap:
        copy.start()
    rings = {}
    for direction in range(2):
        if has(1, direction, 0):
            rings[1, direction, 0] = ring_copies(1, direction, 0)
            for copy in rings[1, direction, 0]:
                copy.start()
    spread = []
    for i, device in enumerate(group):
        copy = remote(x_ref, x_block(half, row, side), x_send.at[i], x_recv.at[i], device)
        copy.start()
        spread.append(copy)
    locals_ = [
        pltpu.make_async_copy(x_ref, x_block(half, row, side), local_sem.at[0]),
        pltpu.make_async_copy(wp_ref.at[half], wp_out.at[sp], local_sem.at[1]),
        pltpu.make_async_copy(wo_ref.at[half], wo_out.at[sp], local_sem.at[2]),
    ]
    for copy in locals_:
        copy.start()
    share = [remote(x_ref, x_block(half, row, side), s_send.at[0], s_recv.at[0], sibling)]
    share[0].start()

    for copy in swap:
        copy.wait_recv()
    for direction in range(2):
        if has(1, direction, 1):
            rings[1, direction, 1] = ring_copies(1, direction, 1)
            for copy in rings[1, direction, 1]:
                copy.start()

    def advance(k):
        for item in range(2):
            for direction in range(2):
                if has(k, direction, item):
                    for copy in rings[k - 1, direction, item]:
                        copy.wait_recv()
                    rings[k, direction, item] = ring_copies(k, direction, item)
                    for copy in rings[k, direction, item]:
                        copy.start()
                elif has(k - 1, direction, item):
                    for copy in rings[k - 1, direction, item]:
                        copy.wait_recv()
            if k == 2 and item == 0:
                pass_on()

    def pass_on():
        for i, (a, b) in enumerate(offsets):
            spread[i].wait_recv()
            block = x_block(lax.rem(half + 2 - a, 2), lax.rem(row + tall - b, tall), side)
            copy = remote(block, block, s_send.at[i + 1], s_recv.at[i + 1], sibling)
            copy.start()
            share.append(copy)

    for k in range(2, steps + 1):
        advance(k)
    if steps < 2:
        pass_on()
    for direction in range(2):
        for item in range(2):
            if has(steps, direction, item):
                for copy in rings[steps, direction, item]:
                    copy.wait_recv()
    for copy in share:
        copy.wait_recv()
    for copy in locals_:
        copy.wait()
    for copy in swap + spread + share + [c for copies in rings.values() for c in copies]:
        copy.wait_send()


def gather_all(rows_in, packed, packed_out):
    pairs, tall = lax.axis_size("sp") // 2, lax.axis_size("tp") // 2
    any_space = pl.BlockSpec(memory_space=pl.ANY)
    vmem = pl.BlockSpec(memory_space=pltpu.VMEM)
    dma = pltpu.SemaphoreType.DMA
    steps = pairs // 2
    return pl.pallas_call(
        functools.partial(gather_kernel, pairs, tall),
        out_shape=(
            jax.ShapeDtypeStruct(
                (2, rows_in.shape[0], rows_in.shape[1] * 2 * tall), rows_in.dtype
            ),
            jax.ShapeDtypeStruct((2 * pairs,) + packed.shape[1:], packed.dtype),
            jax.ShapeDtypeStruct((2 * pairs,) + packed_out.shape[1:], packed_out.dtype),
        ),
        in_specs=[vmem] * 3,
        out_specs=[any_space] * 3,
        scratch_shapes=[
            dma((3,)),
            dma((2 * tall,)), dma((2 * tall,)),
            dma((2 * tall,)), dma((2 * tall,)),
            dma((2,)), dma((2,)),
            dma((steps * 4, 2)), dma((steps * 4, 2)),
        ],
        compiler_params=pltpu.CompilerParams(collective_id=0, has_side_effects=True),
    )(rows_in, packed, packed_out)


def merge_kernel(
    tall, mix_ref, w_ref, out_ref, give, got, total, send, recv, d_send, d_recv
):
    sp, tp = lax.axis_index("sp"), lax.axis_index("tp")
    pair, half = sp // 2, sp % 2
    row, side = tp // 2, tp % 2
    height = out_ref.shape[0]
    places = [(a, b) for a in range(2) for b in range(tall)][::-1]
    count = len(places)
    sibling = (sp, 2 * row + 1 - side)

    def target(a, b):
        return (lax.rem(half + a, 2), lax.rem(row + b, tall))

    barrier = pltpu.get_barrier_semaphore()
    greeted = [sibling]
    for a, b in places[:-1]:
        h, r = target(a, b)
        greeted.append((2 * pair + h, 2 * r + side))
    for device in greeted:
        pl.semaphore_signal(barrier, inc=1, device_id=device, device_id_type=MESH)

    def product(a, b, s):
        h, r = target(a, b)
        start = pl.multiple_of(((h * tall + r) * 2 + s) * height, height)
        return jnp.dot(
            mix_ref[pl.ds(start, height), :], w_ref[...], preferred_element_type=jnp.float32
        )

    crossed = []
    for i, (a, b) in enumerate(places):
        give[i] = product(a, b, 1 - side).astype(give.dtype)
        if i == 0:
            pl.semaphore_wait(barrier, len(greeted))
        copy = remote(give.at[i], got.at[i], d_send.at[i], d_recv.at[i], sibling)
        copy.start()
        crossed.append(copy)
    sent = []
    for i, (a, b) in enumerate(places):
        mine = product(a, b, side)
        crossed[i].wait_recv()
        mine = mine + got[i].astype(jnp.float32)
        if i < count - 1:
            h, r = target(a, b)
            give[count + i] = mine.astype(give.dtype)
            copy = remote(
                give.at[count + i], got.at[count + i], send.at[i], recv.at[i],
                (2 * pair + h, 2 * r + side),
            )
            copy.start()
            sent.append(copy)
        else:
            total[...] = mine
    for i, copy in enumerate(sent):
        copy.wait_recv()
        total[...] += got[count + i].astype(jnp.float32)
    out_ref[...] = total[...].astype(out_ref.dtype)
    for copy in crossed + sent:
        copy.wait_send()


def merged_output(mix, weight, height):
    tall = lax.axis_size("tp") // 2
    vmem = pl.BlockSpec(memory_space=pltpu.VMEM)
    dma = pltpu.SemaphoreType.DMA
    slots = 4 * tall - 1
    width = weight.shape[1]
    return pl.pallas_call(
        functools.partial(merge_kernel, tall),
        out_shape=jax.ShapeDtypeStruct((height, width), jnp.bfloat16),
        in_specs=[vmem] * 2,
        out_specs=vmem,
        scratch_shapes=[
            pltpu.VMEM((slots, height, width), jnp.bfloat16),
            pltpu.VMEM((slots, height, width), jnp.bfloat16),
            pltpu.VMEM((height, width), jnp.float32),
            dma((2 * tall,)), dma((2 * tall,)), dma((2 * tall,)), dma((2 * tall,)),
        ],
        compiler_params=pltpu.CompilerParams(
            collective_id=1, has_side_effects=True, vmem_limit_bytes=48 * 2**20
        ),
    )(mix, weight)


def shifted_pairs(block, distance):
    size = lax.axis_size("sp")
    route = [(i - 2 * distance, i) for i in range(size) if i - 2 * distance >= 0]
    return lax.ppermute(block, "sp", route)


def causal_taps(padded, taps):
    span_rows = padded.shape[0] - taps.shape[0] + 1
    running = jnp.zeros((span_rows, padded.shape[1]), jnp.float32)
    for lag_index in range(taps.shape[0]):
        running = running + taps[lag_index] * padded[lag_index : lag_index + span_rows].astype(
            jnp.float32
        )
    return running


def local(
    inputs,
    norm_gain,
    query_weight,
    key_weight,
    value_weight,
    outgate_weight,
    inputgate_weight,
    forget_weight,
    forget_bias,
    conv_query,
    conv_key,
    cell_gain,
    pool_weight,
    group_weight,
    pool_gain,
    cell_out_weight,
    pool_out_weight,
):
    f32, bf16 = jnp.float32, jnp.bfloat16
    sp_index, tp_index = lax.axis_index("sp"), lax.axis_index("tp")
    n_sp = lax.axis_size("sp")
    pairs = n_sp // 2
    pair, half = sp_index // 2, sp_index % 2
    tokens_here = inputs.shape[0]
    span = 2 * tokens_here
    local_heads = forget_bias.shape[0]
    head = query_weight.shape[1] // 2
    group = pool_weight.shape[1] // 2

    def halves(array, axis):
        return jnp.split(array, 2, axis=axis)

    ingredients = [
        halves(w, 1)
        for w in (query_weight, key_weight, value_weight, outgate_weight, pool_weight)
    ]
    packed = jnp.stack([jnp.concatenate([w[j] for w in ingredients], axis=1) for j in range(2)])
    cell_halves, pool_halves = halves(cell_out_weight, 0), halves(pool_out_weight, 0)
    packed_out = jnp.stack(
        [jnp.concatenate([cell_halves[j], pool_halves[j]], axis=0) for j in range(2)]
    )
    gain_rows = jnp.broadcast_to(norm_gain[None, :], (16, norm_gain.shape[0]))
    rows_in = jnp.concatenate([inputs, gain_rows], axis=0)
    x_all, w_all, wo_all = gather_all(rows_in, packed, packed_out)

    whole_weight = w_all.reshape(-1, w_all.shape[2])
    whole_out = wo_all.transpose(1, 0, 2).reshape(wo_all.shape[1], -1)
    whole_gain = x_all[0, tokens_here]
    whole_wide = x_all[:, :tokens_here].reshape(span, -1).astype(f32)
    features = whole_wide.shape[1]
    squares = jnp.sum(whole_wide * whole_wide, axis=1, keepdims=True)
    normed = (whole_wide * whole_gain.astype(f32)).astype(bf16)
    inverse_rms = lax.rsqrt(squares / features + epsilon)
    pre = (jnp.dot(normed, whole_weight, preferred_element_type=f32) * inverse_rms).astype(bf16)

    head_index = tp_index * local_heads + half
    gate_cols = jnp.concatenate(
        [
            lax.dynamic_slice_in_dim(inputgate_weight, head_index, 1, 1),
            lax.dynamic_slice_in_dim(forget_weight, head_index, 1, 1),
        ],
        axis=1,
    )
    gates = jnp.dot(normed, gate_cols, preferred_element_type=f32) * inverse_rms
    sequence_log = math.log(tokens_here * n_sp)
    log_in = gates[:, 0].reshape(2, tokens_here)
    log_keep = jax.nn.log_sigmoid(gates[:, 1] + forget_bias[half] + sequence_log)
    log_keep = log_keep.reshape(2, tokens_here)

    def own(array, axis, width):
        return lax.dynamic_slice_in_dim(array, half * width, width, axis)

    widest = 2**LEVELS - 1
    edges = jnp.concatenate([pre[-widest:, : 2 * head], pre[-widest:, 4 * head :]], axis=1)
    before = shifted_pairs(edges, 1)
    margin = conv_query.shape[0] - 1
    qk_taps = causal_taps(
        jnp.concatenate([before[widest - margin :, : 2 * head], pre[:, : 2 * head]], axis=0),
        jnp.concatenate([own(conv_query, 1, head), own(conv_key, 1, head)], axis=1),
    )
    qk = jax.nn.silu(qk_taps)
    queries = (qk[:, :head] * head ** (-0.5)).astype(bf16).reshape(2, tokens_here, head)
    key_rows = qk[:, head:].astype(bf16).reshape(2, tokens_here, head)
    value_rows = pre[:, 2 * head : 3 * head].reshape(2, tokens_here, head)
    outgate_pre = pre[:, 3 * head : 4 * head]
    pool_pre = pre[:, 4 * head :]

    cumulative = jnp.cumsum(log_keep, axis=1)
    final = cumulative[:, -1]
    lead = final[:, None] - cumulative + log_in
    own_ceiling = jnp.max(lead, axis=1)
    share = jnp.exp(lead - own_ceiling[:, None])
    weighted = (value_rows.astype(f32) * share[:, :, None]).astype(bf16)
    memory = jnp.einsum("csv,csk->cvk", weighted, key_rows, preferred_element_type=f32)
    normal = jnp.sum(share[:, :, None] * key_rows.astype(f32), axis=1)
    both_ceiling = jnp.maximum(final[1] + own_ceiling[0], own_ceiling[1])
    first = jnp.exp(final[1] + own_ceiling[0] - both_ceiling)
    second = jnp.exp(own_ceiling[1] - both_ceiling)
    state = jnp.concatenate(
        [
            first * memory[0] + second * memory[1],
            (first * normal[0] + second * normal[1])[None],
            jnp.broadcast_to(both_ceiling, (1, head)),
            jnp.broadcast_to(final[0] + final[1], (1, head)),
            jnp.zeros((5, head), f32),
        ],
        axis=0,
    )
    arrived = [shifted_pairs(state, d) for d in range(1, pairs)]
    later = jnp.zeros((), f32)
    logs = []
    for d, block in enumerate(arrived, 1):
        logs.append(jnp.where(d <= pair, block[head + 1, 0] + later, big_negative))
        later = later + block[head + 2, 0]
    ceiling_in = functools.reduce(jnp.maximum, logs)
    total = jnp.zeros((head + 1, head), f32)
    for d, block in enumerate(arrived, 1):
        factor = jnp.where(d <= pair, jnp.exp(logs[d - 1] - ceiling_in), 0.0)
        total = total + factor * block[: head + 1]
    memory_in, normal_in = total[:head], total[head]
    next_ceiling = jnp.maximum(final[0] + ceiling_in, own_ceiling[0])
    kept = jnp.exp(final[0] + ceiling_in - next_ceiling)
    added = jnp.exp(own_ceiling[0] - next_ceiling)
    memories = jnp.stack([memory_in, kept * memory_in + added * memory[0]])
    normals = jnp.stack([normal_in, kept * normal_in + added * normal[0]])
    ceilings = jnp.stack([ceiling_in, next_ceiling])

    causal = jnp.arange(tokens_here)[:, None] >= jnp.arange(tokens_here)[None, :]
    decay_log = cumulative[:, :, None] - cumulative[:, None, :] + log_in[:, None, :]
    decay_log = jnp.where(causal[None], decay_log, -jnp.inf)
    carried_log = cumulative + ceilings[:, None]
    ceiling = jnp.maximum(carried_log, jnp.max(decay_log, axis=2))
    within = jnp.exp(decay_log - ceiling[:, :, None])
    carried = jnp.exp(carried_log - ceiling)
    raw = jnp.einsum("ctd,csd->cts", queries, key_rows, preferred_element_type=f32)
    scores = (raw * within).astype(bf16)
    query_wide = queries.astype(f32)
    numerator = carried[:, :, None] * jnp.einsum(
        "ctk,cvk->ctv", query_wide, memories, precision=highest
    )
    numerator = numerator + jnp.einsum(
        "cts,csv->ctv", scores, value_rows, preferred_element_type=f32
    )
    denominator = carried * jnp.sum(query_wide * normals[:, None, :], axis=2) + jnp.sum(
        scores.astype(f32), axis=2
    )
    hidden = numerator / jnp.maximum(jnp.abs(denominator), jnp.exp(-ceiling))[:, :, None]
    normalized = hidden * lax.rsqrt(jnp.mean(hidden * hidden, axis=2, keepdims=True) + epsilon)
    cell_mix = (
        normalized.reshape(span, head)
        * own(cell_gain, 0, head)
        * jax.nn.sigmoid(outgate_pre.astype(f32))
    ).astype(bf16)

    group_index = tp_index * group_weight.shape[0] + half
    level = group_index % LEVELS
    running = jnp.concatenate([before[:, 2 * head :], pool_pre], axis=0).astype(f32)
    window_sum = None
    for step in range(LEVELS):
        running = running[2**step :] + running[: -(2**step)]
        window = running[running.shape[0] - span :]
        window_sum = window if step == 0 else jnp.where(level >= step, window, window_sum)
    reach = (2 ** (1 + level)).astype(jnp.int32)
    row_ids = pair * span + jnp.arange(span, dtype=jnp.int32)
    counted = jnp.minimum(row_ids + 1, reach).astype(f32)
    pooled = (window_sum / counted[:, None] - pool_pre.astype(f32)).astype(bf16)
    own_group = lax.dynamic_index_in_dim(group_weight, half, 0, keepdims=False)
    pool_mix = (
        jnp.dot(pooled, own_group, preferred_element_type=f32) * own(pool_gain, 0, group)
    ).astype(bf16)

    mix = jnp.concatenate([cell_mix, pool_mix], axis=1)
    return merged_output(mix, whole_out, tokens_here // lax.axis_size("tp"))


def solution(mesh):
    in_specs = (
        P("sp", "tp"),
        P("tp"),
        P("sp", "tp"),
        P("sp", "tp"),
        P("sp", "tp"),
        P("sp", "tp"),
        P(),
        P(),
        P("tp"),
        P(None, "tp"),
        P(None, "tp"),
        P("tp"),
        P("sp", "tp"),
        P("tp", None, None),
        P("tp"),
        P("tp", "sp"),
        P("tp", "sp"),
    )
    out_specs = P(("sp", "tp"), None)
    return jax.shard_map(local, mesh=mesh, in_specs=in_specs, out_specs=out_specs, check_vma=False)
```

```python
import functools
import math

import jax
import jax.numpy as jnp
from jax import lax
from jax.experimental import pallas as pl
from jax.experimental.pallas import tpu as pltpu
from jax.sharding import PartitionSpec as P

LEVELS = 4

epsilon = 1e-06
big_negative = -1e30
highest = lax.Precision.HIGHEST
MESH = pl.DeviceIdType.MESH


def remote(src, dst, send, recv, device):
    return pltpu.make_async_remote_copy(
        src_ref=src, dst_ref=dst, send_sem=send, recv_sem=recv,
        device_id=device, device_id_type=MESH,
    )


def gather_kernel(
    pairs, tall, x_ref, wp_ref, wo_ref, x_out, wp_out, wo_out,
    local_sem, x_send, x_recv, s_send, s_recv, h_send, h_recv, r_send, r_recv,
):
    sp, tp = lax.axis_index("sp"), lax.axis_index("tp")
    pair, half = sp // 2, sp % 2
    row, side = tp // 2, tp % 2
    width = x_ref.shape[1]
    other = 2 * pair + 1 - half
    sibling = (sp, 2 * row + 1 - side)
    right = (2 * lax.rem(pair + 1, pairs) + half, tp)
    left = (2 * lax.rem(pair + pairs - 1, pairs) + half, tp)
    offsets = [(a, b) for a in range(2) for b in range(tall) if (a, b) != (0, 0)]
    group = [
        (2 * pair + lax.rem(half + a, 2), 2 * lax.rem(row + b, tall) + side) for a, b in offsets
    ]

    barrier = pltpu.get_barrier_semaphore()
    greeted = group + [sibling, right, left]
    for device in greeted:
        pl.semaphore_signal(barrier, inc=1, device_id=device, device_id_type=MESH)
    pl.semaphore_wait(barrier, len(greeted))

    def x_block(h, r, s):
        column = pl.multiple_of((2 * r + s) * width, width)
        return x_out.at[h, :, pl.ds(column, width)]

    def ring_copies(k, direction, item):
        if direction == 0:
            source = lax.rem(pair - k + 1 + pairs, pairs)
        else:
            source = lax.rem(pair + k - 1, pairs)
        place = 2 * source + (half if item == 0 else 1 - half)
        target = right if direction == 0 else left
        own = k == 1 and item == 0
        index = ((k - 1) * 2 + direction) * 2 + item
        out = []
        for j, (whole, mine) in enumerate(((wp_out, wp_ref), (wo_out, wo_ref))):
            src = mine.at[half] if own else whole.at[place]
            out.append(
                remote(src, whole.at[place], r_send.at[index, j], r_recv.at[index, j], target)
            )
        return out

    steps = pairs // 2

    def has(k, direction, item):
        return k < steps or (k == steps and direction == item)

    swap = [
        remote(wp_ref.at[1 - half], wp_out.at[sp], h_send.at[0], h_recv.at[0], (other, tp)),
        remote(wo_ref.at[1 - half], wo_out.at[sp], h_send.at[1], h_recv.at[1], (other, tp)),
    ]
    for copy in swap:
        copy.start()
    rings = {}
    for direction in range(2):
        if has(1, direction, 0):
            rings[1, direction, 0] = ring_copies(1, direction, 0)
            for copy in rings[1, direction, 0]:
                copy.start()
    spread = []
    for i, device in enumerate(group):
        copy = remote(x_ref, x_block(half, row, side), x_send.at[i], x_recv.at[i], device)
        copy.start()
        spread.append(copy)
    locals_ = [
        pltpu.make_async_copy(x_ref, x_block(half, row, side), local_sem.at[0]),
        pltpu.make_async_copy(wp_ref.at[half], wp_out.at[sp], local_sem.at[1]),
        pltpu.make_async_copy(wo_ref.at[half], wo_out.at[sp], local_sem.at[2]),
    ]
    for copy in locals_:
        copy.start()
    share = [remote(x_ref, x_block(half, row, side), s_send.at[0], s_recv.at[0], sibling)]
    share[0].start()

    for copy in swap:
        copy.wait_recv()
    for direction in range(2):
        if has(1, direction, 1):
            rings[1, direction, 1] = ring_copies(1, direction, 1)
            for copy in rings[1, direction, 1]:
                copy.start()

    def advance(k):
        for item in range(2):
            for direction in range(2):
                if has(k, direction, item):
                    for copy in rings[k - 1, direction, item]:
                        copy.wait_recv()
                    rings[k, direction, item] = ring_copies(k, direction, item)
                    for copy in rings[k, direction, item]:
                        copy.start()
                elif has(k - 1, direction, item):
                    for copy in rings[k - 1, direction, item]:
                        copy.wait_recv()
            if k == 2 and item == 0:
                pass_on()

    def pass_on():
        for i, (a, b) in enumerate(offsets):
            spread[i].wait_recv()
            block = x_block(lax.rem(half + 2 - a, 2), lax.rem(row + tall - b, tall), side)
            copy = remote(block, block, s_send.at[i + 1], s_recv.at[i + 1], sibling)
            copy.start()
            share.append(copy)

    for k in range(2, steps + 1):
        advance(k)
    if steps < 2:
        pass_on()
    for direction in range(2):
        for item in range(2):
            if has(steps, direction, item):
                for copy in rings[steps, direction, item]:
                    copy.wait_recv()
    for copy in share:
        copy.wait_recv()
    for copy in locals_:
        copy.wait()
    for copy in swap + spread + share + [c for copies in rings.values() for c in copies]:
        copy.wait_send()


def gather_all(rows_in, packed, packed_out):
    pairs, tall = lax.axis_size("sp") // 2, lax.axis_size("tp") // 2
    any_space = pl.BlockSpec(memory_space=pl.ANY)
    vmem = pl.BlockSpec(memory_space=pltpu.VMEM)
    dma = pltpu.SemaphoreType.DMA
    steps = pairs // 2
    return pl.pallas_call(
        functools.partial(gather_kernel, pairs, tall),
        out_shape=(
            jax.ShapeDtypeStruct(
                (2, rows_in.shape[0], rows_in.shape[1] * 2 * tall), rows_in.dtype
            ),
            jax.ShapeDtypeStruct((2 * pairs,) + packed.shape[1:], packed.dtype),
            jax.ShapeDtypeStruct((2 * pairs,) + packed_out.shape[1:], packed_out.dtype),
        ),
        in_specs=[vmem] * 3,
        out_specs=[any_space] * 3,
        scratch_shapes=[
            dma((3,)),
            dma((2 * tall,)), dma((2 * tall,)),
            dma((2 * tall,)), dma((2 * tall,)),
            dma((2,)), dma((2,)),
            dma((steps * 4, 2)), dma((steps * 4, 2)),
        ],
        compiler_params=pltpu.CompilerParams(collective_id=0, has_side_effects=True),
    )(rows_in, packed, packed_out)


def columns_of(rows):
    filled = jnp.concatenate(
        rows + [jnp.zeros((128 - len(rows), rows[0].shape[1]), jnp.float32)], axis=0
    )
    return filled.T


def scanned(row, combine, fill):
    length = row.shape[1]
    lane = lax.broadcasted_iota(jnp.int32, (8, length), 1)
    value = jnp.broadcast_to(row, (8, length))
    step = 1
    while step < length:
        moved = pltpu.roll(value, step, 1)
        value = combine(value, jnp.where(lane >= step, moved, fill))
        step *= 2
    return value[:1]


def cell_kernel(
    pairs, tall, head, group,
    pre_ref, gate_ref, taps_ref, gain_ref, group_ref, pool_gain_ref, w_ref, out_ref,
    edge_q, edge_p, ext, ext_p, q_s, k_s, num_s, small_s, mix_s, st, st_in,
    give, got, total, edge_sem, state_send, state_recv, send, recv, d_send, d_recv,
):
    f32, bf16 = jnp.float32, jnp.bfloat16
    sp, tp = lax.axis_index("sp"), lax.axis_index("tp")
    pair, half = sp // 2, sp % 2
    row, side = tp // 2, tp % 2
    height = out_ref.shape[0]
    span = pre_ref.shape[0]
    length = span // 2
    places = [(a, b) for a in range(2) for b in range(tall)][::-1]
    count = len(places)
    sibling = (sp, 2 * row + 1 - side)

    def target(a, b):
        return (lax.rem(half + a, 2), lax.rem(row + b, tall))

    barrier = pltpu.get_barrier_semaphore()
    greeted = [sibling]
    for a, b in places[:-1]:
        h, r = target(a, b)
        greeted.append((2 * pair + h, 2 * r + side))
    for d in range(1, pairs):
        greeted.append((2 * lax.rem(pair + d, pairs) + half, tp))
    for device in greeted:
        pl.semaphore_signal(barrier, inc=1, device_id=device, device_id_type=MESH)
    pl.semaphore_wait(barrier, len(greeted))

    following = (2 * lax.rem(pair + 1, pairs) + half, tp)
    edges = [
        remote(pre_ref.at[pl.ds(span - 16, 16), pl.ds(0, 2 * head)], edge_q,
               edge_sem.at[0], edge_sem.at[1], following),
        remote(pre_ref.at[pl.ds(span - 16, 16), pl.ds(4 * head, group)], edge_p,
               edge_sem.at[2], edge_sem.at[3], following),
    ]

    @pl.when(pair < pairs - 1)
    def _():
        for copy in edges:
            copy.start()

    @pl.when(pair == 0)
    def _():
        edge_q[...] = jnp.zeros_like(edge_q)
        edge_p[...] = jnp.zeros_like(edge_p)

    ext[pl.ds(16, span), :] = pre_ref[:, : 2 * head].astype(f32)
    ext_p[pl.ds(16, span), :] = pre_ref[:, 4 * head :].astype(f32)

    finals, tops, leads, gaps, cols = [], [], [], [], []
    for c in range(2):
        log_in = gate_ref[pl.ds(c, 1), :]
        cumulative = scanned(gate_ref[pl.ds(2 + c, 1), :], jnp.add, 0.0)
        gap = log_in - cumulative
        ceiling = scanned(gap, jnp.maximum, big_negative)
        final = cumulative[:, length - 1 :]
        top = final + ceiling[:, length - 1 :]
        share = jnp.exp(final + gap - top)
        finals.append(final)
        tops.append(top)
        gaps.append(gap)
        cols.append(columns_of([cumulative, ceiling, share]))

    @pl.when(pair > 0)
    def _():
        for copy in edges:
            copy.wait_recv()

    ext[pl.ds(0, 16), :] = edge_q[...].astype(f32)
    ext_p[pl.ds(0, 16), :] = edge_p[...].astype(f32)

    taps = taps_ref.shape[0]
    for c in range(2):
        running = None
        for j in range(taps):
            term = taps_ref[pl.ds(j, 1), :] * ext[pl.ds(16 + c * length - taps + 1 + j, length), :]
            running = term if running is None else running + term
        active = running * jax.nn.sigmoid(running)
        q_s[pl.ds(c * length, length), :] = (active[:, :head] * head ** (-0.5)).astype(bf16)
        k_s[pl.ds(c * length, length), :] = active[:, head:].astype(bf16)

    memories, normals = [], []
    for c in range(2):
        share = cols[c][:, 2:3]
        keys = k_s[pl.ds(c * length, length), :]
        values = pre_ref[pl.ds(c * length, length), pl.ds(2 * head, head)].astype(f32)
        memories.append(
            lax.dot_general(
                (values * share).astype(bf16), keys, (((0,), (0,)), ((), ())),
                preferred_element_type=f32,
            )
        )
        normals.append(jnp.sum(keys.astype(f32) * share, axis=0, keepdims=True))
    both = jnp.maximum(finals[1] + tops[0], tops[1])
    first, second = jnp.exp(finals[1] + tops[0] - both), jnp.exp(tops[1] - both)
    st[pl.ds(0, head), :] = first * memories[0] + second * memories[1]
    st[pl.ds(head, 8), :] = jnp.concatenate(
        [
            first * normals[0] + second * normals[1],
            jnp.broadcast_to(both, (1, head)),
            jnp.broadcast_to(finals[0] + finals[1], (1, head)),
            jnp.zeros((5, head), f32),
        ],
        axis=0,
    )
    states = []
    for d in range(1, pairs):
        copy = remote(
            st, st_in.at[d - 1], state_send.at[d - 1], state_recv.at[d - 1],
            (2 * lax.rem(pair + d, pairs) + half, tp),
        )
        states.append(copy)
        pl.when(pair + d < pairs)(copy.start)

        @pl.when(pair < d)
        def _():
            st_in[d - 1] = jnp.zeros(st_in.shape[1:], f32)

    block = 128 if length % 128 == 0 else length
    for c in range(2):
        for t in range(0, length, block):
            reach = t + block
            scores = lax.dot_general(
                q_s[pl.ds(c * length + t, block), :], k_s[pl.ds(c * length, reach), :],
                (((1,), (1,)), ((), ())), preferred_element_type=f32,
            )
            weight = jnp.exp(
                jnp.minimum(gaps[c][:, :reach] - cols[c][t : t + block, 1:2], 0.0)
            )
            t_ids = t + lax.broadcasted_iota(jnp.int32, (block, reach), 0)
            s_ids = lax.broadcasted_iota(jnp.int32, (block, reach), 1)
            scores = jnp.where(t_ids >= s_ids, scores * weight, 0.0).astype(bf16)
            num_s[pl.ds(c * length + t, block), :] = jnp.dot(
                scores, pre_ref[pl.ds(c * length, reach), pl.ds(2 * head, head)],
                preferred_element_type=f32,
            )
            small_s[pl.ds(c * length + t, block), :] = jnp.broadcast_to(
                jnp.sum(scores.astype(f32), axis=1, keepdims=True), (block, 128)
            )

    level = (tp * 2 + half) % LEVELS
    window = None
    for step in range(LEVELS):
        low, high = (0, 2) if step == 0 else (2**step, 2 ** (step + 1))
        part = ext_p[pl.ds(16 - low, span), :]
        for lag in range(low + 1, high):
            part = part + ext_p[pl.ds(16 - lag, span), :]
        if window is None:
            window = part
        else:
            window = window + jnp.where(level >= step, part, 0.0)
    reach = lax.shift_left(jnp.int32(2), level.astype(jnp.int32))
    row_ids = pair * span + lax.broadcasted_iota(jnp.int32, (span, group), 0)
    counted = jnp.minimum(row_ids + 1, reach).astype(f32)
    pooled = (window / counted - ext_p[pl.ds(16, span), :]).astype(bf16)
    mix_s[:, head:] = (
        jnp.dot(pooled, group_ref[...], preferred_element_type=f32) * pool_gain_ref[...]
    ).astype(bf16)

    later = jnp.zeros((1, 1), f32)
    logs = []
    for d in range(1, pairs):
        pl.when(pair >= d)(states[d - 1].wait_recv)
        logs.append(jnp.where(pair >= d, st_in[d - 1, head + 1 : head + 2, :1] + later, big_negative))
        later = later + st_in[d - 1, head + 2 : head + 3, :1]
    ceiling_in = functools.reduce(jnp.maximum, logs)
    memory_in = jnp.zeros((head, head), f32)
    normal_in = jnp.zeros((1, head), f32)
    for d in range(1, pairs):
        factor = jnp.where(pair >= d, jnp.exp(logs[d - 1] - ceiling_in), 0.0)
        memory_in = memory_in + factor * st_in[d - 1, :head, :]
        normal_in = normal_in + factor * st_in[d - 1, head : head + 1, :]
    for c in range(2):
        high = memory_in.astype(bf16)
        low = (memory_in - high.astype(f32)).astype(bf16)
        here = pl.ds(c * length, length)
        queries = q_s[here, :]
        over = (((1,), (1,)), ((), ()))
        far = lax.dot_general(queries, high, over, preferred_element_type=f32)
        far = far + lax.dot_general(queries, low, over, preferred_element_type=f32)
        far_sum = jnp.sum(queries.astype(f32) * normal_in, axis=1, keepdims=True)
        cum, near_top = cols[c][:, 0:1], cols[c][:, 1:2]
        near_log, far_log = cum + near_top, cum + ceiling_in
        ceiling = jnp.maximum(near_log, far_log)
        near_scale, far_scale = jnp.exp(near_log - ceiling), jnp.exp(far_log - ceiling)
        numerator = near_scale * num_s[here, :] + far_scale * far
        denominator = near_scale * small_s[here, :1] + far_scale * far_sum
        hidden = numerator / jnp.maximum(jnp.abs(denominator), jnp.exp(-ceiling))
        hidden = hidden * lax.rsqrt(jnp.mean(hidden * hidden, axis=1, keepdims=True) + epsilon)
        gate = jax.nn.sigmoid(pre_ref[here, pl.ds(3 * head, head)].astype(f32))
        mix_s[here, :head] = (hidden * gain_ref[...] * gate).astype(bf16)
        if c == 0:
            upper = jnp.maximum(finals[0] + ceiling_in, tops[0])
            kept, added = jnp.exp(finals[0] + ceiling_in - upper), jnp.exp(tops[0] - upper)
            memory_in = kept * memory_in + added * memories[0]
            normal_in = kept * normal_in + added * normals[0]
            ceiling_in = upper

    def product(a, b, s):
        h, r = target(a, b)
        start = pl.multiple_of(((h * tall + r) * 2 + s) * height, height)
        return jnp.dot(
            mix_s[pl.ds(start, height), :], w_ref[...], preferred_element_type=f32
        )

    crossed = []
    for i, (a, b) in enumerate(places):
        give[i] = product(a, b, 1 - side).astype(give.dtype)
        copy = remote(give.at[i], got.at[i], d_send.at[i], d_recv.at[i], sibling)
        copy.start()
        crossed.append(copy)
    sent = []
    for i, (a, b) in enumerate(places):
        mine = product(a, b, side)
        crossed[i].wait_recv()
        mine = mine + got[i].astype(f32)
        if i < count - 1:
            h, r = target(a, b)
            give[count + i] = mine.astype(give.dtype)
            copy = remote(
                give.at[count + i], got.at[count + i], send.at[i], recv.at[i],
                (2 * pair + h, 2 * r + side),
            )
            copy.start()
            sent.append(copy)
        else:
            total[...] = mine
    for i, copy in enumerate(sent):
        copy.wait_recv()
        total[...] += got[count + i].astype(f32)
    out_ref[...] = total[...].astype(out_ref.dtype)
    for copy in crossed + sent:
        copy.wait_send()
    for d in range(1, pairs):
        pl.when(pair + d < pairs)(states[d - 1].wait_send)

    @pl.when(pair < pairs - 1)
    def _():
        for copy in edges:
            copy.wait_send()


def cell_and_merge(pre, gates, taps, gain, own_group, pool_gain, weight, height):
    pairs, tall = lax.axis_size("sp") // 2, lax.axis_size("tp") // 2
    f32, bf16 = jnp.float32, jnp.bfloat16
    vmem = pl.BlockSpec(memory_space=pltpu.VMEM)
    dma = pltpu.SemaphoreType.DMA
    slots = 4 * tall - 1
    width = weight.shape[1]
    span, head, group = pre.shape[0], gain.shape[1], pool_gain.shape[1]
    return pl.pallas_call(
        functools.partial(cell_kernel, pairs, tall, head, group),
        out_shape=jax.ShapeDtypeStruct((height, width), bf16),
        in_specs=[vmem] * 7,
        out_specs=vmem,
        scratch_shapes=[
            pltpu.VMEM((16, 2 * head), bf16),
            pltpu.VMEM((16, group), bf16),
            pltpu.VMEM((span + 16, 2 * head), f32),
            pltpu.VMEM((span + 16, group), f32),
            pltpu.VMEM((span, head), bf16),
            pltpu.VMEM((span, head), bf16),
            pltpu.VMEM((span, head), f32),
            pltpu.VMEM((span, 128), f32),
            pltpu.VMEM((span, head + group), bf16),
            pltpu.VMEM((head + 8, head), f32),
            pltpu.VMEM((pairs - 1, head + 8, head), f32),
            pltpu.VMEM((slots, height, width), bf16),
            pltpu.VMEM((slots, height, width), bf16),
            pltpu.VMEM((height, width), f32),
            dma((4,)), dma((pairs - 1,)), dma((pairs - 1,)),
            dma((2 * tall,)), dma((2 * tall,)), dma((2 * tall,)), dma((2 * tall,)),
        ],
        compiler_params=pltpu.CompilerParams(
            collective_id=1, has_side_effects=True, vmem_limit_bytes=56 * 2**20
        ),
    )(pre, gates, taps, gain, own_group, pool_gain, weight)


def local(
    inputs,
    norm_gain,
    query_weight,
    key_weight,
    value_weight,
    outgate_weight,
    inputgate_weight,
    forget_weight,
    forget_bias,
    conv_query,
    conv_key,
    cell_gain,
    pool_weight,
    group_weight,
    pool_gain,
    cell_out_weight,
    pool_out_weight,
):
    f32, bf16 = jnp.float32, jnp.bfloat16
    sp_index, tp_index = lax.axis_index("sp"), lax.axis_index("tp")
    n_sp = lax.axis_size("sp")
    pairs = n_sp // 2
    pair, half = sp_index // 2, sp_index % 2
    tokens_here = inputs.shape[0]
    span = 2 * tokens_here
    local_heads = forget_bias.shape[0]
    head = query_weight.shape[1] // 2
    group = pool_weight.shape[1] // 2

    def halves(array, axis):
        return jnp.split(array, 2, axis=axis)

    ingredients = [
        halves(w, 1)
        for w in (query_weight, key_weight, value_weight, outgate_weight, pool_weight)
    ]
    packed = jnp.stack([jnp.concatenate([w[j] for w in ingredients], axis=1) for j in range(2)])
    cell_halves, pool_halves = halves(cell_out_weight, 0), halves(pool_out_weight, 0)
    packed_out = jnp.stack(
        [jnp.concatenate([cell_halves[j], pool_halves[j]], axis=0) for j in range(2)]
    )
    gain_rows = jnp.broadcast_to(norm_gain[None, :], (16, norm_gain.shape[0]))
    rows_in = jnp.concatenate([inputs, gain_rows], axis=0)
    x_all, w_all, wo_all = gather_all(rows_in, packed, packed_out)

    whole_weight = w_all.reshape(-1, w_all.shape[2])
    whole_out = wo_all.transpose(1, 0, 2).reshape(wo_all.shape[1], -1)
    whole_gain = x_all[0, tokens_here]
    whole_wide = x_all[:, :tokens_here].reshape(span, -1).astype(f32)
    features = whole_wide.shape[1]
    squares = jnp.sum(whole_wide * whole_wide, axis=1, keepdims=True)
    normed = (whole_wide * whole_gain.astype(f32)).astype(bf16)
    inverse_rms = lax.rsqrt(squares / features + epsilon)
    pre = (jnp.dot(normed, whole_weight, preferred_element_type=f32) * inverse_rms).astype(bf16)

    head_index = tp_index * local_heads + half
    gate_cols = jnp.concatenate(
        [
            lax.dynamic_slice_in_dim(inputgate_weight, head_index, 1, 1),
            lax.dynamic_slice_in_dim(forget_weight, head_index, 1, 1),
        ],
        axis=1,
    )
    gates = lax.dot_general(
        gate_cols, normed, (((0,), (1,)), ((), ())), preferred_element_type=f32
    ) * inverse_rms.reshape(1, span)
    sequence_log = math.log(tokens_here * n_sp)
    log_in = gates[0].reshape(2, tokens_here)
    log_keep = jax.nn.log_sigmoid(gates[1] + forget_bias[half] + sequence_log)
    gate_rows = jnp.concatenate(
        [log_in, log_keep.reshape(2, tokens_here), jnp.zeros((4, tokens_here), f32)], axis=0
    )

    def own(array, axis, width):
        return lax.dynamic_slice_in_dim(array, half * width, width, axis)

    taps = jnp.concatenate([own(conv_query, 1, head), own(conv_key, 1, head)], axis=1)
    own_group = lax.dynamic_index_in_dim(group_weight, half, 0, keepdims=False)
    return cell_and_merge(
        pre,
        gate_rows,
        taps,
        own(cell_gain, 0, head)[None],
        own_group,
        own(pool_gain, 0, group)[None],
        whole_out,
        tokens_here // lax.axis_size("tp"),
    )


def solution(mesh):
    in_specs = (
        P("sp", "tp"),
        P("tp"),
        P("sp", "tp"),
        P("sp", "tp"),
        P("sp", "tp"),
        P("sp", "tp"),
        P(),
        P(),
        P("tp"),
        P(None, "tp"),
        P(None, "tp"),
        P("tp"),
        P("sp", "tp"),
        P("tp", None, None),
        P("tp"),
        P("tp", "sp"),
        P("tp", "sp"),
    )
    out_specs = P(("sp", "tp"), None)
    return jax.shard_map(local, mesh=mesh, in_specs=in_specs, out_specs=out_specs, check_vma=False)
```

```python
import functools
import math

import jax
import jax.numpy as jnp
from jax import lax
from jax.experimental import pallas as pl
from jax.experimental.pallas import tpu as pltpu
from jax.sharding import PartitionSpec as P

LEVELS = 4

epsilon = 1e-06
big_negative = -1e30
highest = lax.Precision.HIGHEST
MESH = pl.DeviceIdType.MESH


def remote(src, dst, send, recv, device):
    return pltpu.make_async_remote_copy(
        src_ref=src, dst_ref=dst, send_sem=send, recv_sem=recv,
        device_id=device, device_id_type=MESH,
    )


def columns_of(rows):
    filled = jnp.concatenate(
        rows + [jnp.zeros((128 - len(rows), rows[0].shape[1]), jnp.float32)], axis=0
    )
    return filled.T


def scanned(row, combine, fill):
    length = row.shape[1]
    lane = lax.broadcasted_iota(jnp.int32, (8, length), 1)
    value = jnp.broadcast_to(row, (8, length))
    step = 1
    while step < length:
        moved = pltpu.roll(value, step, 1)
        value = combine(value, jnp.where(lane >= step, moved, fill))
        step *= 2
    return value[:1]


def mixer_kernel(
    pairs, tall, tokens, head, group,
    x_ref, wp_ref, wo_ref, gatew_ref, bias_ref, taps_ref, gain_ref, group_ref, pool_gain_ref,
    out_ref,
    x_out, wp_out, wo_out, normed, inv_s, raw_gate, acc, pre_ref, w_ref,
    edge_q, edge_p, ext, ext_p, q_s, k_s, num_s, small_s, mix_s, st, st_low, st_in, low_in,
    give, got, total,
    local_sem, x_send, x_recv, s_send, s_recv, h_send, h_recv, r_send, r_recv,
    edge_sem, state_send, state_recv, send, recv, d_send, d_recv,
):
    f32, bf16 = jnp.float32, jnp.bfloat16
    height = out_ref.shape[0]
    span = 2 * tokens
    length = tokens
    features = x_out.shape[2]
    sp, tp = lax.axis_index("sp"), lax.axis_index("tp")
    pair, half = sp // 2, sp % 2
    row, side = tp // 2, tp % 2
    width = x_ref.shape[1]
    other = 2 * pair + 1 - half
    sibling = (sp, 2 * row + 1 - side)
    right = (2 * lax.rem(pair + 1, pairs) + half, tp)
    left = (2 * lax.rem(pair + pairs - 1, pairs) + half, tp)
    offsets = [(a, b) for a in range(2) for b in range(tall) if (a, b) != (0, 0)]
    peers = [
        (2 * pair + lax.rem(half + a, 2), 2 * lax.rem(row + b, tall) + side) for a, b in offsets
    ]

    places = [(a, b) for a in range(2) for b in range(tall)][::-1]
    count = len(places)

    def target(a, b):
        return (lax.rem(half + a, 2), lax.rem(row + b, tall))

    barrier = pltpu.get_barrier_semaphore()
    greeted = [sibling]
    for a, b in places[:-1]:
        h, r = target(a, b)
        greeted.append((2 * pair + h, 2 * r + side))
    for d in range(1, pairs):
        greeted.append((2 * lax.rem(pair + d, pairs) + half, tp))
    for device in greeted:
        pl.semaphore_signal(barrier, inc=1, device_id=device, device_id_type=MESH)
    pl.semaphore_wait(barrier, len(greeted))

    def x_block(h, r, s):
        column = pl.multiple_of((2 * r + s) * width, width)
        return x_out.at[h, :, pl.ds(column, width)]

    def ring_copies(k, direction, item):
        if direction == 0:
            source = lax.rem(pair - k + 1 + pairs, pairs)
        else:
            source = lax.rem(pair + k - 1, pairs)
        place = 2 * source + (half if item == 0 else 1 - half)
        target = right if direction == 0 else left
        own = k == 1 and item == 0
        index = ((k - 1) * 2 + direction) * 2 + item
        out = []
        for j, (whole, mine) in enumerate(((wp_out, wp_ref), (wo_out, wo_ref))):
            src = mine.at[half] if own else whole.at[place]
            out.append(
                remote(src, whole.at[place], r_send.at[index, j], r_recv.at[index, j], target)
            )
        return out

    steps = pairs // 2

    def has(k, direction, item):
        return k < steps or (k == steps and direction == item)

    swap = [
        remote(wp_ref.at[1 - half], wp_out.at[sp], h_send.at[0], h_recv.at[0], (other, tp)),
        remote(wo_ref.at[1 - half], wo_out.at[sp], h_send.at[1], h_recv.at[1], (other, tp)),
    ]
    for copy in swap:
        copy.start()
    rings = {}
    for direction in range(2):
        if has(1, direction, 0):
            rings[1, direction, 0] = ring_copies(1, direction, 0)
            for copy in rings[1, direction, 0]:
                copy.start()
    spread = []
    for i, device in enumerate(peers):
        copy = remote(x_ref, x_block(half, row, side), x_send.at[i], x_recv.at[i], device)
        copy.start()
        spread.append(copy)
    locals_ = [
        pltpu.make_async_copy(x_ref, x_block(half, row, side), local_sem.at[0]),
        pltpu.make_async_copy(wp_ref.at[half], wp_out.at[sp], local_sem.at[1]),
        pltpu.make_async_copy(wo_ref.at[half], wo_out.at[sp], local_sem.at[2]),
    ]
    for copy in locals_:
        copy.start()
    passed = [remote(x_ref, x_block(half, row, side), s_send.at[0], s_recv.at[0], sibling)]
    passed[0].start()

    acc[...] = jnp.zeros_like(acc)
    for copy in swap:
        copy.wait_recv()
    for direction in range(2):
        if has(1, direction, 1):
            rings[1, direction, 1] = ring_copies(1, direction, 1)
            for copy in rings[1, direction, 1]:
                copy.start()

    def advance(k):
        for item in range(2):
            for direction in range(2):
                if has(k, direction, item):
                    for copy in rings[k - 1, direction, item]:
                        copy.wait_recv()
                    rings[k, direction, item] = ring_copies(k, direction, item)
                    for copy in rings[k, direction, item]:
                        copy.start()
                elif has(k - 1, direction, item):
                    for copy in rings[k - 1, direction, item]:
                        copy.wait_recv()
            if k == 2 and item == 0:
                pass_on()

    def pass_on():
        for i, (a, b) in enumerate(offsets):
            spread[i].wait_recv()
            block = x_block(lax.rem(half + 2 - a, 2), lax.rem(row + tall - b, tall), side)
            copy = remote(block, block, s_send.at[i + 1], s_recv.at[i + 1], sibling)
            copy.start()
            passed.append(copy)

    for k in range(2, steps + 1):
        advance(k)
    if steps < 2:
        pass_on()
    for copy in passed:
        copy.wait_recv()
    for copy in locals_:
        copy.wait()

    whole_gain = x_out[0, tokens : tokens + 1, :].astype(f32)
    small_rows = 128 if tokens % 128 == 0 else tokens
    for h in range(2):
        @pl.loop(0, tokens // small_rows)
        def _(i):
            start = pl.multiple_of(i * small_rows, small_rows)
            wide = x_out[h, pl.ds(start, small_rows), :].astype(f32)
            squares = jnp.sum(wide * wide, axis=1, keepdims=True)
            there = pl.ds(h * tokens + start, small_rows)
            normed[there, :] = (wide * whole_gain).astype(bf16)
            inverse = lax.rsqrt(squares / features + epsilon)
            inv_s[there, :] = jnp.broadcast_to(inverse, (small_rows, 128))

    big_rows = 256 if span % 256 == 0 else span
    depth = wp_ref.shape[1]
    by_item = depth % 128 == 0

    def add_product(place):
        if by_item:
            @pl.loop(0, span // big_rows)
            def _(i):
                there = pl.ds(pl.multiple_of(i * big_rows, big_rows), big_rows)
                across = pl.ds(pl.multiple_of(place * depth, depth), depth)
                acc[there, :] += jnp.dot(
                    normed[there, across], wp_out[place], preferred_element_type=f32
                )

    @pl.loop(0, span // big_rows)
    def _(i):
        there = pl.ds(pl.multiple_of(i * big_rows, big_rows), big_rows)
        raw_gate[there, :] = inv_s[there, :] * jnp.dot(
            normed[there, :], gatew_ref[...], preferred_element_type=f32
        )

    def arrived_place(k, direction, item):
        source = lax.rem(pair - k + pairs, pairs) if direction == 0 else lax.rem(pair + k, pairs)
        return 2 * source + (half if item == 0 else 1 - half)

    add_product(sp)
    add_product(other)
    for k in range(1, steps):
        for direction in range(2):
            for item in range(2):
                add_product(arrived_place(k, direction, item))
    for direction in range(2):
        for item in range(2):
            if has(steps, direction, item):
                for copy in rings[steps, direction, item][:1]:
                    copy.wait_recv()
                add_product(arrived_place(steps, direction, item))

    @pl.loop(0, span // big_rows)
    def _(i):
        there = pl.ds(pl.multiple_of(i * big_rows, big_rows), big_rows)
        if by_item:
            product_here = acc[there, :]
        else:
            weights = wp_out[...].reshape(-1, wp_out.shape[2])
            product_here = jnp.dot(normed[there, :], weights, preferred_element_type=f32)
        pre_ref[there, :] = (product_here * inv_s[there, :1]).astype(bf16)

    gate_t = raw_gate[...].T
    keep = gate_t[1:2, :] + bias_ref[:, :1]
    small = jnp.exp(-jnp.abs(keep))
    ratio = small / (2.0 + small)
    square = ratio * ratio
    series = jnp.full_like(square, 1.0 / 17.0)
    for odd in (15, 13, 11, 9, 7, 5, 3, 1):
        series = series * square + 1.0 / odd
    log_keep_row = jnp.minimum(keep, 0.0) - 2.0 * ratio * series
    log_in_row = gate_t[0:1, :]

    following = (2 * lax.rem(pair + 1, pairs) + half, tp)
    edges = [
        remote(pre_ref.at[pl.ds(span - 16, 16), pl.ds(0, 2 * head)], edge_q,
               edge_sem.at[0], edge_sem.at[1], following),
        remote(pre_ref.at[pl.ds(span - 16, 16), pl.ds(4 * head, group)], edge_p,
               edge_sem.at[2], edge_sem.at[3], following),
    ]

    @pl.when(pair < pairs - 1)
    def _():
        for copy in edges:
            copy.start()

    @pl.when(pair == 0)
    def _():
        edge_q[...] = jnp.zeros_like(edge_q)
        edge_p[...] = jnp.zeros_like(edge_p)

    ext[pl.ds(16, span), :] = pre_ref[:, : 2 * head].astype(f32)
    ext_p[pl.ds(16, span), :] = pre_ref[:, 4 * head :].astype(f32)

    finals, tops, leads, gaps, cols = [], [], [], [], []
    for c in range(2):
        log_in = log_in_row[:, c * length : (c + 1) * length]
        cumulative = scanned(log_keep_row[:, c * length : (c + 1) * length], jnp.add, 0.0)
        gap = log_in - cumulative
        ceiling = scanned(gap, jnp.maximum, big_negative)
        final = cumulative[:, length - 1 :]
        top = final + ceiling[:, length - 1 :]
        share = jnp.exp(final + gap - top)
        finals.append(final)
        tops.append(top)
        gaps.append(gap)
        cols.append(columns_of([cumulative, ceiling, share]))

    @pl.when(pair > 0)
    def _():
        for copy in edges:
            copy.wait_recv()

    ext[pl.ds(0, 16), :] = edge_q[...].astype(f32)
    ext_p[pl.ds(0, 16), :] = edge_p[...].astype(f32)

    taps = taps_ref.shape[0]
    for c in range(2):
        running = None
        for j in range(taps):
            term = taps_ref[pl.ds(j, 1), :] * ext[pl.ds(16 + c * length - taps + 1 + j, length), :]
            running = term if running is None else running + term
        active = running * jax.nn.sigmoid(running)
        q_s[pl.ds(c * length, length), :] = (active[:, :head] * head ** (-0.5)).astype(bf16)
        k_s[pl.ds(c * length, length), :] = active[:, head:].astype(bf16)

    memories, normals = [], []
    for c in range(2):
        share = cols[c][:, 2:3]
        keys = k_s[pl.ds(c * length, length), :]
        values = pre_ref[pl.ds(c * length, length), pl.ds(2 * head, head)].astype(f32)
        memories.append(
            lax.dot_general(
                (values * share).astype(bf16), keys, (((0,), (0,)), ((), ())),
                preferred_element_type=f32,
            )
        )
        normals.append(jnp.sum(keys.astype(f32) * share, axis=0, keepdims=True))
    both = jnp.maximum(finals[1] + tops[0], tops[1])
    first, second = jnp.exp(finals[1] + tops[0] - both), jnp.exp(tops[1] - both)
    st[...] = (first * memories[0] + second * memories[1]).astype(bf16)
    st_low[...] = jnp.concatenate(
        [
            first * normals[0] + second * normals[1],
            jnp.broadcast_to(both, (1, head)),
            jnp.broadcast_to(finals[0] + finals[1], (1, head)),
            jnp.zeros((5, head), f32),
        ],
        axis=0,
    )
    states = []
    for d in range(1, pairs):
        to = (2 * lax.rem(pair + d, pairs) + half, tp)
        copies = [
            remote(st, st_in.at[d - 1], state_send.at[d - 1, 0], state_recv.at[d - 1, 0], to),
            remote(
                st_low, low_in.at[d - 1], state_send.at[d - 1, 1], state_recv.at[d - 1, 1], to
            ),
        ]
        states.append(copies)
        for copy in copies:
            pl.when(pair + d < pairs)(copy.start)

        @pl.when(pair < d)
        def _():
            st_in[d - 1] = jnp.zeros(st_in.shape[1:], bf16)
            low_in[d - 1] = jnp.zeros(low_in.shape[1:], f32)

    block = 128 if length % 128 == 0 else length
    for c in range(2):
        for t in range(0, length, block):
            reach = t + block
            scores = lax.dot_general(
                q_s[pl.ds(c * length + t, block), :], k_s[pl.ds(c * length, reach), :],
                (((1,), (1,)), ((), ())), preferred_element_type=f32,
            )
            weight = jnp.exp(
                jnp.minimum(gaps[c][:, :reach] - cols[c][t : t + block, 1:2], 0.0)
            )
            t_ids = t + lax.broadcasted_iota(jnp.int32, (block, reach), 0)
            s_ids = lax.broadcasted_iota(jnp.int32, (block, reach), 1)
            scores = jnp.where(t_ids >= s_ids, scores * weight, 0.0).astype(bf16)
            num_s[pl.ds(c * length + t, block), :] = jnp.dot(
                scores, pre_ref[pl.ds(c * length, reach), pl.ds(2 * head, head)],
                preferred_element_type=f32,
            )
            small_s[pl.ds(c * length + t, block), :] = jnp.broadcast_to(
                jnp.sum(scores.astype(f32), axis=1, keepdims=True), (block, 128)
            )

    level = (tp * 2 + half) % LEVELS
    window = None
    for step in range(LEVELS):
        low, high = (0, 2) if step == 0 else (2**step, 2 ** (step + 1))
        part = ext_p[pl.ds(16 - low, span), :]
        for lag in range(low + 1, high):
            part = part + ext_p[pl.ds(16 - lag, span), :]
        if window is None:
            window = part
        else:
            window = window + jnp.where(level >= step, part, 0.0)
    reach = lax.shift_left(jnp.int32(2), level.astype(jnp.int32))
    row_ids = pair * span + lax.broadcasted_iota(jnp.int32, (span, group), 0)
    counted = jnp.minimum(row_ids + 1, reach).astype(f32)
    pooled = (window / counted - ext_p[pl.ds(16, span), :]).astype(bf16)
    mix_s[:, head:] = (
        jnp.dot(pooled, group_ref[...], preferred_element_type=f32) * pool_gain_ref[...]
    ).astype(bf16)

    later = jnp.zeros((1, 1), f32)
    logs = []
    for d in range(1, pairs):
        for copy in states[d - 1]:
            pl.when(pair >= d)(copy.wait_recv)
        logs.append(jnp.where(pair >= d, low_in[d - 1, 1:2, :1] + later, big_negative))
        later = later + low_in[d - 1, 2:3, :1]
    ceiling_in = functools.reduce(jnp.maximum, logs)
    memory_in = jnp.zeros((head, head), f32)
    normal_in = jnp.zeros((1, head), f32)
    for d in range(1, pairs):
        factor = jnp.where(pair >= d, jnp.exp(logs[d - 1] - ceiling_in), 0.0)
        memory_in = memory_in + factor * st_in[d - 1].astype(f32)
        normal_in = normal_in + factor * low_in[d - 1, 0:1, :]
    for c in range(2):
        high = memory_in.astype(bf16)
        low = (memory_in - high.astype(f32)).astype(bf16)
        here = pl.ds(c * length, length)
        queries = q_s[here, :]
        over = (((1,), (1,)), ((), ()))
        far = lax.dot_general(queries, high, over, preferred_element_type=f32)
        far = far + lax.dot_general(queries, low, over, preferred_element_type=f32)
        far_sum = jnp.sum(queries.astype(f32) * normal_in, axis=1, keepdims=True)
        cum, near_top = cols[c][:, 0:1], cols[c][:, 1:2]
        near_log, far_log = cum + near_top, cum + ceiling_in
        ceiling = jnp.maximum(near_log, far_log)
        near_scale, far_scale = jnp.exp(near_log - ceiling), jnp.exp(far_log - ceiling)
        numerator = near_scale * num_s[here, :] + far_scale * far
        denominator = near_scale * small_s[here, :1] + far_scale * far_sum
        hidden = numerator / jnp.maximum(jnp.abs(denominator), jnp.exp(-ceiling))
        hidden = hidden * lax.rsqrt(jnp.mean(hidden * hidden, axis=1, keepdims=True) + epsilon)
        gate = jax.nn.sigmoid(pre_ref[here, pl.ds(3 * head, head)].astype(f32))
        mix_s[here, :head] = (hidden * gain_ref[...] * gate).astype(bf16)
        if c == 0:
            upper = jnp.maximum(finals[0] + ceiling_in, tops[0])
            kept, added = jnp.exp(finals[0] + ceiling_in - upper), jnp.exp(tops[0] - upper)
            memory_in = kept * memory_in + added * memories[0]
            normal_in = kept * normal_in + added * normals[0]
            ceiling_in = upper

    for direction in range(2):
        for item in range(2):
            if has(steps, direction, item):
                for copy in rings[steps, direction, item][1:]:
                    copy.wait_recv()
    columns = wo_out.shape[2]
    for s in range(wo_out.shape[0]):
        w_ref[:, s * columns : (s + 1) * columns] = wo_out[s]

    def product(a, b, s):
        h, r = target(a, b)
        start = pl.multiple_of(((h * tall + r) * 2 + s) * height, height)
        return jnp.dot(
            mix_s[pl.ds(start, height), :], w_ref[...], preferred_element_type=f32
        )

    crossed = []
    for i, (a, b) in enumerate(places):
        give[i] = product(a, b, 1 - side).astype(give.dtype)
        copy = remote(give.at[i], got.at[i], d_send.at[i], d_recv.at[i], sibling)
        copy.start()
        crossed.append(copy)
    sent = []
    for i, (a, b) in enumerate(places):
        mine = product(a, b, side)
        crossed[i].wait_recv()
        mine = mine + got[i].astype(f32)
        if i < count - 1:
            h, r = target(a, b)
            give[count + i] = mine.astype(give.dtype)
            copy = remote(
                give.at[count + i], got.at[count + i], send.at[i], recv.at[i],
                (2 * pair + h, 2 * r + side),
            )
            copy.start()
            sent.append(copy)
        else:
            total[...] = mine
    for i, copy in enumerate(sent):
        copy.wait_recv()
        total[...] += got[count + i].astype(f32)
    out_ref[...] = total[...].astype(out_ref.dtype)
    for copy in crossed + sent:
        copy.wait_send()
    for d in range(1, pairs):
        for copy in states[d - 1]:
            pl.when(pair + d < pairs)(copy.wait_send)

    @pl.when(pair < pairs - 1)
    def _():
        for copy in edges:
            copy.wait_send()

    for copy in swap + spread + passed + [c for copies in rings.values() for c in copies]:
        copy.wait_send()


def mixed_rows(rows_in, packed, packed_out, gate_weight, bias, taps, gain, own_group, pool_gain):
    pairs, n_tp = lax.axis_size("sp") // 2, lax.axis_size("tp")
    tall = n_tp // 2
    f32, bf16 = jnp.float32, jnp.bfloat16
    vmem = pl.BlockSpec(memory_space=pltpu.VMEM)
    dma = pltpu.SemaphoreType.DMA
    slots, steps = 4 * tall - 1, pairs // 2
    head, group = gain.shape[1], pool_gain.shape[1]
    tokens = rows_in.shape[0] - 16
    span, features, height = 2 * tokens, rows_in.shape[1] * n_tp, tokens // n_tp
    width = packed_out.shape[2] * 2 * pairs
    scratch = [
        ((2, rows_in.shape[0], features), bf16),
        ((2 * pairs,) + packed.shape[1:], bf16),
        ((2 * pairs,) + packed_out.shape[1:], bf16),
        ((span, features), bf16),
        ((span, 128), f32),
        ((span, 128), f32),
        ((span, packed.shape[2]), f32),
        ((span, packed.shape[2]), bf16),
        ((head + group, width), bf16),
        ((16, 2 * head), bf16),
        ((16, group), bf16),
        ((span + 16, 2 * head), f32),
        ((span + 16, group), f32),
        ((span, head), bf16),
        ((span, head), bf16),
        ((span, head), f32),
        ((span, 128), f32),
        ((span, head + group), bf16),
        ((head, head), bf16),
        ((8, head), f32),
        ((pairs - 1, head, head), bf16),
        ((pairs - 1, 8, head), f32),
        ((slots, height, width), bf16),
        ((slots, height, width), bf16),
        ((height, width), f32),
    ]
    return pl.pallas_call(
        functools.partial(mixer_kernel, pairs, tall, tokens, head, group),
        out_shape=jax.ShapeDtypeStruct((height, width), bf16),
        in_specs=[vmem] * 9,
        out_specs=vmem,
        scratch_shapes=[pltpu.VMEM(shape, kind) for shape, kind in scratch] + [
            dma((3,)),
            dma((2 * tall,)), dma((2 * tall,)),
            dma((2 * tall,)), dma((2 * tall,)),
            dma((2,)), dma((2,)),
            dma((steps * 4, 2)), dma((steps * 4, 2)),
            dma((4,)), dma((pairs - 1, 2)), dma((pairs - 1, 2)),
            dma((2 * tall,)), dma((2 * tall,)), dma((2 * tall,)), dma((2 * tall,)),
        ],
        compiler_params=pltpu.CompilerParams(
            collective_id=0, has_side_effects=True, vmem_limit_bytes=63 * 2**20
        ),
    )(rows_in, packed, packed_out, gate_weight, bias, taps, gain, own_group, pool_gain)


def local(
    inputs,
    norm_gain,
    query_weight,
    key_weight,
    value_weight,
    outgate_weight,
    inputgate_weight,
    forget_weight,
    forget_bias,
    conv_query,
    conv_key,
    cell_gain,
    pool_weight,
    group_weight,
    pool_gain,
    cell_out_weight,
    pool_out_weight,
):
    f32, bf16 = jnp.float32, jnp.bfloat16
    sp_index, tp_index = lax.axis_index("sp"), lax.axis_index("tp")
    n_sp = lax.axis_size("sp")
    pairs = n_sp // 2
    pair, half = sp_index // 2, sp_index % 2
    tokens_here = inputs.shape[0]
    span = 2 * tokens_here
    local_heads = forget_bias.shape[0]
    head = query_weight.shape[1] // 2
    group = pool_weight.shape[1] // 2

    def halves(array, axis):
        return jnp.split(array, 2, axis=axis)

    ingredients = [
        halves(w, 1)
        for w in (query_weight, key_weight, value_weight, outgate_weight, pool_weight)
    ]
    packed = jnp.stack([jnp.concatenate([w[j] for w in ingredients], axis=1) for j in range(2)])
    cell_halves, pool_halves = halves(cell_out_weight, 0), halves(pool_out_weight, 0)
    packed_out = jnp.stack(
        [jnp.concatenate([cell_halves[j], pool_halves[j]], axis=0) for j in range(2)]
    )
    gain_rows = jnp.broadcast_to(norm_gain[None, :], (16, norm_gain.shape[0]))
    rows_in = jnp.concatenate([inputs, gain_rows], axis=0)
    head_index = tp_index * local_heads + half
    gate_cols = jnp.concatenate(
        [
            lax.dynamic_slice_in_dim(inputgate_weight, head_index, 1, 1),
            lax.dynamic_slice_in_dim(forget_weight, head_index, 1, 1),
        ],
        axis=1,
    )
    gate_weight = jnp.pad(gate_cols, ((0, 0), (0, 126)))
    sequence_log = math.log(tokens_here * n_sp)
    bias = jnp.broadcast_to(forget_bias[half] + sequence_log, (1, 128))

    def own(array, axis, width):
        return lax.dynamic_slice_in_dim(array, half * width, width, axis)

    taps = jnp.concatenate([own(conv_query, 1, head), own(conv_key, 1, head)], axis=1)
    own_group = lax.dynamic_index_in_dim(group_weight, half, 0, keepdims=False)
    return mixed_rows(
        rows_in,
        packed,
        packed_out,
        gate_weight,
        bias,
        taps,
        own(cell_gain, 0, head)[None],
        own_group,
        own(pool_gain, 0, group)[None],
    )


def solution(mesh):
    in_specs = (
        P("sp", "tp"),
        P("tp"),
        P("sp", "tp"),
        P("sp", "tp"),
        P("sp", "tp"),
        P("sp", "tp"),
        P(),
        P(),
        P("tp"),
        P(None, "tp"),
        P(None, "tp"),
        P("tp"),
        P("sp", "tp"),
        P("tp", None, None),
        P("tp"),
        P("tp", "sp"),
        P("tp", "sp"),
    )
    out_specs = P(("sp", "tp"), None)
    return jax.shard_map(local, mesh=mesh, in_specs=in_specs, out_specs=out_specs, check_vma=False)
```

```python
import functools
import math

import jax
import jax.numpy as jnp
from jax import lax
from jax.experimental import pallas as pl
from jax.experimental.pallas import tpu as pltpu
from jax.sharding import PartitionSpec as P

LEVELS = 4

epsilon = 1e-06
big_negative = -1e30
highest = lax.Precision.HIGHEST
MESH = pl.DeviceIdType.MESH


def remote(src, dst, send, recv, device):
    return pltpu.make_async_remote_copy(
        src_ref=src, dst_ref=dst, send_sem=send, recv_sem=recv,
        device_id=device, device_id_type=MESH,
    )


def columns_of(rows):
    filled = jnp.concatenate(
        rows + [jnp.zeros((128 - len(rows), rows[0].shape[1]), jnp.float32)], axis=0
    )
    return filled.T


def scanned(row, combine, fill):
    length = row.shape[1]
    lane = lax.broadcasted_iota(jnp.int32, (8, length), 1)
    value = jnp.broadcast_to(row, (8, length))
    step = 1
    while step < length:
        moved = pltpu.roll(value, step, 1)
        value = combine(value, jnp.where(lane >= step, moved, fill))
        step *= 2
    return value[:1]


def mixer_kernel(
    pairs, tall, tokens, head, group,
    x_ref, wq_ref, wk_ref, wv_ref, wg_ref, wl_ref, co_ref, po_ref, gatew_ref, bias_ref, taps_ref, gain_ref, group_ref, pool_gain_ref,
    out_ref,
    x_out, wp_out, wo_out, normed, inv_s, raw_gate, acc, pre_ref, w_ref,
    edge_q, edge_p, ext, ext_p, q_s, k_s, num_s, small_s, mix_s, st, st_low, st_in, low_in,
    give, got, total,
    local_sem, x_send, x_recv, s_send, s_recv, h_send, h_recv, r_send, r_recv,
    edge_sem, state_send, state_recv, send, recv, d_send, d_recv,
):
    f32, bf16 = jnp.float32, jnp.bfloat16
    height = out_ref.shape[0]
    span = 2 * tokens
    length = tokens
    features = x_out.shape[2]
    sp, tp = lax.axis_index("sp"), lax.axis_index("tp")
    pair, half = sp // 2, sp % 2
    row, side = tp // 2, tp % 2
    width = x_ref.shape[1]
    other = 2 * pair + 1 - half
    sibling = (sp, 2 * row + 1 - side)
    right = (2 * lax.rem(pair + 1, pairs) + half, tp)
    left = (2 * lax.rem(pair + pairs - 1, pairs) + half, tp)
    offsets = [(a, b) for a in range(2) for b in range(tall) if (a, b) != (0, 0)]
    peers = [
        (2 * pair + lax.rem(half + a, 2), 2 * lax.rem(row + b, tall) + side) for a, b in offsets
    ]

    places = [(a, b) for a in range(2) for b in range(tall)][::-1]
    count = len(places)

    def target(a, b):
        return (lax.rem(half + a, 2), lax.rem(row + b, tall))

    barrier = pltpu.get_barrier_semaphore()
    greeted = [sibling]
    for a, b in places[:-1]:
        h, r = target(a, b)
        greeted.append((2 * pair + h, 2 * r + side))
    for d in range(1, pairs):
        greeted.append((2 * lax.rem(pair + d, pairs) + half, tp))
    for device in greeted:
        pl.semaphore_signal(barrier, inc=1, device_id=device, device_id_type=MESH)
    pl.semaphore_wait(barrier, len(greeted))

    def x_block(h, r, s):
        column = pl.multiple_of((2 * r + s) * width, width)
        return x_out.at[h, :, pl.ds(column, width)]

    def ring_copies(k, direction, item, j=0):
        if direction == 0:
            source = lax.rem(pair - k + 1 + pairs, pairs)
        else:
            source = lax.rem(pair + k - 1, pairs)
        place = 2 * source + (half if item == 0 else 1 - half)
        target = right if direction == 0 else left
        index = ((k - 1) * 2 + direction) * 2 + item
        whole = (wp_out, wo_out)[j]
        return [
            remote(
                whole.at[place], whole.at[place], r_send.at[index, j], r_recv.at[index, j], target
            )
        ]

    steps = pairs // 2

    def has(k, direction, item):
        return k < steps or (k == steps and direction == item)

    def parts(j, place):
        out, offset = [], 0
        for source in (wq_ref, wk_ref, wv_ref, wg_ref, wl_ref):
            wide = source.shape[1] // 2
            out.append((
                source.at[:, pl.ds(pl.multiple_of(j * wide, wide), wide)],
                wp_out.at[place, :, pl.ds(offset, wide)],
            ))
            offset += wide
        offset = 0
        for source in (co_ref, po_ref):
            deep = source.shape[0] // 2
            out.append((
                source.at[pl.ds(pl.multiple_of(j * deep, deep), deep), :],
                wo_out.at[place, pl.ds(offset, deep), :],
            ))
            offset += deep
        return out

    loads = [
        pltpu.make_async_copy(src, dst, local_sem.at[i + 1])
        for i, (src, dst) in enumerate(parts(half, sp))
    ]
    for copy in loads:
        copy.start()
    swap = [
        remote(src, dst, h_send.at[i], h_recv.at[i], (other, tp))
        for i, (src, dst) in enumerate(parts(1 - half, sp))
    ]
    for copy in swap:
        copy.start()
    for copy in loads:
        copy.wait()
    rings = {}
    for direction in range(2):
        if has(1, direction, 0):
            rings[1, direction, 0] = ring_copies(1, direction, 0)
            for copy in rings[1, direction, 0]:
                copy.start()
    spread = []
    for i, device in enumerate(peers):
        copy = remote(x_ref, x_block(half, row, side), x_send.at[i], x_recv.at[i], device)
        copy.start()
        spread.append(copy)
    locals_ = [pltpu.make_async_copy(x_ref, x_block(half, row, side), local_sem.at[0])]
    for copy in locals_:
        copy.start()
    passed = [remote(x_ref, x_block(half, row, side), s_send.at[0], s_recv.at[0], sibling)]
    passed[0].start()

    acc[...] = jnp.zeros_like(acc)
    for copy in swap:
        copy.wait_recv()
    for direction in range(2):
        if has(1, direction, 1):
            rings[1, direction, 1] = ring_copies(1, direction, 1)
            for copy in rings[1, direction, 1]:
                copy.start()

    def advance(k):
        for item in range(2):
            for direction in range(2):
                if has(k, direction, item):
                    for copy in rings[k - 1, direction, item]:
                        copy.wait_recv()
                    rings[k, direction, item] = ring_copies(k, direction, item)
                    for copy in rings[k, direction, item]:
                        copy.start()
                elif has(k - 1, direction, item):
                    for copy in rings[k - 1, direction, item]:
                        copy.wait_recv()
            if k == 2 and item == 0:
                pass_on()

    def pass_on():
        for i, (a, b) in enumerate(offsets):
            spread[i].wait_recv()
            block = x_block(lax.rem(half + 2 - a, 2), lax.rem(row + tall - b, tall), side)
            copy = remote(block, block, s_send.at[i + 1], s_recv.at[i + 1], sibling)
            copy.start()
            passed.append(copy)

    out_rings = {}

    def start_out(k):
        for direction in range(2):
            for item in range(2):
                if k > 1 and has(k - 1, direction, item):
                    for copy in out_rings[k - 1, direction, item]:
                        copy.wait_recv()
                if has(k, direction, item):
                    out_rings[k, direction, item] = ring_copies(k, direction, item, 1)
                    for copy in out_rings[k, direction, item]:
                        copy.start()

    for k in range(2, steps + 1):
        advance(k)
    if steps < 2:
        pass_on()
    for copy in passed:
        copy.wait_recv()
    for copy in locals_:
        copy.wait()

    whole_gain = x_out[0, tokens : tokens + 1, :].astype(f32)
    small_rows = 128 if tokens % 128 == 0 else tokens
    for h in range(2):
        @pl.loop(0, tokens // small_rows)
        def _(i):
            start = pl.multiple_of(i * small_rows, small_rows)
            wide = x_out[h, pl.ds(start, small_rows), :].astype(f32)
            squares = jnp.sum(wide * wide, axis=1, keepdims=True)
            there = pl.ds(h * tokens + start, small_rows)
            normed[there, :] = (wide * whole_gain).astype(bf16)
            inverse = lax.rsqrt(squares / features + epsilon)
            inv_s[there, :] = jnp.broadcast_to(inverse, (small_rows, 128))

    big_rows = 256 if span % 256 == 0 else span
    depth = wp_out.shape[1]
    by_item = depth % 128 == 0

    def add_product(place):
        if by_item:
            @pl.loop(0, span // big_rows)
            def _(i):
                there = pl.ds(pl.multiple_of(i * big_rows, big_rows), big_rows)
                across = pl.ds(pl.multiple_of(place * depth, depth), depth)
                acc[there, :] += jnp.dot(
                    normed[there, across], wp_out[place], preferred_element_type=f32
                )

    @pl.loop(0, span // big_rows)
    def _(i):
        there = pl.ds(pl.multiple_of(i * big_rows, big_rows), big_rows)
        raw_gate[there, :] = inv_s[there, :] * jnp.dot(
            normed[there, :], gatew_ref[...], preferred_element_type=f32
        )

    def arrived_place(k, direction, item):
        source = lax.rem(pair - k + pairs, pairs) if direction == 0 else lax.rem(pair + k, pairs)
        return 2 * source + (half if item == 0 else 1 - half)

    add_product(sp)
    add_product(other)
    for k in range(1, steps):
        for direction in range(2):
            for item in range(2):
                add_product(arrived_place(k, direction, item))
    for direction in range(2):
        for item in range(2):
            if has(steps, direction, item):
                for copy in rings[steps, direction, item][:1]:
                    copy.wait_recv()
                add_product(arrived_place(steps, direction, item))

    @pl.loop(0, span // big_rows)
    def _(i):
        there = pl.ds(pl.multiple_of(i * big_rows, big_rows), big_rows)
        if by_item:
            product_here = acc[there, :]
        else:
            weights = wp_out[...].reshape(-1, wp_out.shape[2])
            product_here = jnp.dot(normed[there, :], weights, preferred_element_type=f32)
        pre_ref[there, :] = (product_here * inv_s[there, :1]).astype(bf16)

    gate_t = raw_gate[...].T
    keep = gate_t[1:2, :] + bias_ref[:, :1]
    small = jnp.exp(-jnp.abs(keep))
    ratio = small / (2.0 + small)
    square = ratio * ratio
    series = jnp.full_like(square, 1.0 / 17.0)
    for odd in (15, 13, 11, 9, 7, 5, 3, 1):
        series = series * square + 1.0 / odd
    log_keep_row = jnp.minimum(keep, 0.0) - 2.0 * ratio * series
    log_in_row = gate_t[0:1, :]

    following = (2 * lax.rem(pair + 1, pairs) + half, tp)
    edges = [
        remote(pre_ref.at[pl.ds(span - 16, 16), pl.ds(0, 2 * head)], edge_q,
               edge_sem.at[0], edge_sem.at[1], following),
        remote(pre_ref.at[pl.ds(span - 16, 16), pl.ds(4 * head, group)], edge_p,
               edge_sem.at[2], edge_sem.at[3], following),
    ]

    @pl.when(pair < pairs - 1)
    def _():
        for copy in edges:
            copy.start()

    start_out(1)

    @pl.when(pair == 0)
    def _():
        edge_q[...] = jnp.zeros_like(edge_q)
        edge_p[...] = jnp.zeros_like(edge_p)

    ext[pl.ds(16, span), :] = pre_ref[:, : 2 * head].astype(f32)
    ext_p[pl.ds(16, span), :] = pre_ref[:, 4 * head :].astype(f32)

    finals, tops, leads, gaps, cols = [], [], [], [], []
    for c in range(2):
        log_in = log_in_row[:, c * length : (c + 1) * length]
        cumulative = scanned(log_keep_row[:, c * length : (c + 1) * length], jnp.add, 0.0)
        gap = log_in - cumulative
        ceiling = scanned(gap, jnp.maximum, big_negative)
        final = cumulative[:, length - 1 :]
        top = final + ceiling[:, length - 1 :]
        share = jnp.exp(final + gap - top)
        finals.append(final)
        tops.append(top)
        gaps.append(gap)
        cols.append(columns_of([cumulative, ceiling, share]))

    @pl.when(pair > 0)
    def _():
        for copy in edges:
            copy.wait_recv()

    ext[pl.ds(0, 16), :] = edge_q[...].astype(f32)
    ext_p[pl.ds(0, 16), :] = edge_p[...].astype(f32)

    taps = taps_ref.shape[0]
    for c in range(2):
        running = None
        for j in range(taps):
            term = taps_ref[pl.ds(j, 1), :] * ext[pl.ds(16 + c * length - taps + 1 + j, length), :]
            running = term if running is None else running + term
        active = running * jax.nn.sigmoid(running)
        q_s[pl.ds(c * length, length), :] = (active[:, :head] * head ** (-0.5)).astype(bf16)
        k_s[pl.ds(c * length, length), :] = active[:, head:].astype(bf16)

    memories, normals = [], []
    for c in range(2):
        share = cols[c][:, 2:3]
        keys = k_s[pl.ds(c * length, length), :]
        values = pre_ref[pl.ds(c * length, length), pl.ds(2 * head, head)].astype(f32)
        memories.append(
            lax.dot_general(
                (values * share).astype(bf16), keys, (((0,), (0,)), ((), ())),
                preferred_element_type=f32,
            )
        )
        normals.append(jnp.sum(keys.astype(f32) * share, axis=0, keepdims=True))
    both = jnp.maximum(finals[1] + tops[0], tops[1])
    first, second = jnp.exp(finals[1] + tops[0] - both), jnp.exp(tops[1] - both)
    st[...] = (first * memories[0] + second * memories[1]).astype(bf16)
    st_low[...] = jnp.concatenate(
        [
            first * normals[0] + second * normals[1],
            jnp.broadcast_to(both, (1, head)),
            jnp.broadcast_to(finals[0] + finals[1], (1, head)),
            jnp.zeros((5, head), f32),
        ],
        axis=0,
    )
    states = []
    for d in range(1, pairs):
        to = (2 * lax.rem(pair + d, pairs) + half, tp)
        copies = [
            remote(st, st_in.at[d - 1], state_send.at[d - 1, 0], state_recv.at[d - 1, 0], to),
            remote(
                st_low, low_in.at[d - 1], state_send.at[d - 1, 1], state_recv.at[d - 1, 1], to
            ),
        ]
        states.append(copies)
        for copy in copies:
            pl.when(pair + d < pairs)(copy.start)

        @pl.when(pair < d)
        def _():
            st_in[d - 1] = jnp.zeros(st_in.shape[1:], bf16)
            low_in[d - 1] = jnp.zeros(low_in.shape[1:], f32)

    block = 128 if length % 128 == 0 else length
    for c in range(2):
        for t in range(0, length, block):
            reach = t + block
            scores = lax.dot_general(
                q_s[pl.ds(c * length + t, block), :], k_s[pl.ds(c * length, reach), :],
                (((1,), (1,)), ((), ())), preferred_element_type=f32,
            )
            weight = jnp.exp(
                jnp.minimum(gaps[c][:, :reach] - cols[c][t : t + block, 1:2], 0.0)
            )
            t_ids = t + lax.broadcasted_iota(jnp.int32, (block, reach), 0)
            s_ids = lax.broadcasted_iota(jnp.int32, (block, reach), 1)
            scores = jnp.where(t_ids >= s_ids, scores * weight, 0.0).astype(bf16)
            num_s[pl.ds(c * length + t, block), :] = jnp.dot(
                scores, pre_ref[pl.ds(c * length, reach), pl.ds(2 * head, head)],
                preferred_element_type=f32,
            )
            small_s[pl.ds(c * length + t, block), :] = jnp.broadcast_to(
                jnp.sum(scores.astype(f32), axis=1, keepdims=True), (block, 128)
            )
        if c == 0 and steps >= 2:
            start_out(2)

    level = (tp * 2 + half) % LEVELS
    window = None
    for step in range(LEVELS):
        low, high = (0, 2) if step == 0 else (2**step, 2 ** (step + 1))
        part = ext_p[pl.ds(16 - low, span), :]
        for lag in range(low + 1, high):
            part = part + ext_p[pl.ds(16 - lag, span), :]
        if window is None:
            window = part
        else:
            window = window + jnp.where(level >= step, part, 0.0)
    reach = lax.shift_left(jnp.int32(2), level.astype(jnp.int32))
    row_ids = pair * span + lax.broadcasted_iota(jnp.int32, (span, group), 0)
    counted = jnp.minimum(row_ids + 1, reach).astype(f32)
    pooled = (window / counted - ext_p[pl.ds(16, span), :]).astype(bf16)
    mix_s[:, head:] = (
        jnp.dot(pooled, group_ref[...], preferred_element_type=f32) * pool_gain_ref[...]
    ).astype(bf16)

    later = jnp.zeros((1, 1), f32)
    logs = []
    for d in range(1, pairs):
        for copy in states[d - 1]:
            pl.when(pair >= d)(copy.wait_recv)
        logs.append(jnp.where(pair >= d, low_in[d - 1, 1:2, :1] + later, big_negative))
        later = later + low_in[d - 1, 2:3, :1]
    ceiling_in = functools.reduce(jnp.maximum, logs)
    memory_in = jnp.zeros((head, head), f32)
    normal_in = jnp.zeros((1, head), f32)
    for d in range(1, pairs):
        factor = jnp.where(pair >= d, jnp.exp(logs[d - 1] - ceiling_in), 0.0)
        memory_in = memory_in + factor * st_in[d - 1].astype(f32)
        normal_in = normal_in + factor * low_in[d - 1, 0:1, :]
    for c in range(2):
        high = memory_in.astype(bf16)
        low = (memory_in - high.astype(f32)).astype(bf16)
        here = pl.ds(c * length, length)
        queries = q_s[here, :]
        over = (((1,), (1,)), ((), ()))
        far = lax.dot_general(queries, high, over, preferred_element_type=f32)
        far = far + lax.dot_general(queries, low, over, preferred_element_type=f32)
        far_sum = jnp.sum(queries.astype(f32) * normal_in, axis=1, keepdims=True)
        cum, near_top = cols[c][:, 0:1], cols[c][:, 1:2]
        near_log, far_log = cum + near_top, cum + ceiling_in
        ceiling = jnp.maximum(near_log, far_log)
        near_scale, far_scale = jnp.exp(near_log - ceiling), jnp.exp(far_log - ceiling)
        numerator = near_scale * num_s[here, :] + far_scale * far
        denominator = near_scale * small_s[here, :1] + far_scale * far_sum
        hidden = numerator / jnp.maximum(jnp.abs(denominator), jnp.exp(-ceiling))
        hidden = hidden * lax.rsqrt(jnp.mean(hidden * hidden, axis=1, keepdims=True) + epsilon)
        gate = jax.nn.sigmoid(pre_ref[here, pl.ds(3 * head, head)].astype(f32))
        mix_s[here, :head] = (hidden * gain_ref[...] * gate).astype(bf16)
        if c == 0:
            upper = jnp.maximum(finals[0] + ceiling_in, tops[0])
            kept, added = jnp.exp(finals[0] + ceiling_in - upper), jnp.exp(tops[0] - upper)
            memory_in = kept * memory_in + added * memories[0]
            normal_in = kept * normal_in + added * normals[0]
            ceiling_in = upper

    for k in range(3, steps + 1):
        start_out(k)
    for direction in range(2):
        for item in range(2):
            if has(steps, direction, item):
                for copy in out_rings[steps, direction, item]:
                    copy.wait_recv()
    columns = wo_out.shape[2]
    for s in range(wo_out.shape[0]):
        w_ref[:, s * columns : (s + 1) * columns] = wo_out[s]

    def product(a, b, s):
        h, r = target(a, b)
        start = pl.multiple_of(((h * tall + r) * 2 + s) * height, height)
        return jnp.dot(
            mix_s[pl.ds(start, height), :], w_ref[...], preferred_element_type=f32
        )

    crossed = []
    for i, (a, b) in enumerate(places):
        give[i] = product(a, b, 1 - side).astype(give.dtype)
        copy = remote(give.at[i], got.at[i], d_send.at[i], d_recv.at[i], sibling)
        copy.start()
        crossed.append(copy)
    sent = []
    for i, (a, b) in enumerate(places):
        mine = product(a, b, side)
        crossed[i].wait_recv()
        mine = mine + got[i].astype(f32)
        if i < count - 1:
            h, r = target(a, b)
            give[count + i] = mine.astype(give.dtype)
            copy = remote(
                give.at[count + i], got.at[count + i], send.at[i], recv.at[i],
                (2 * pair + h, 2 * r + side),
            )
            copy.start()
            sent.append(copy)
        else:
            total[...] = mine
    for i, copy in enumerate(sent):
        copy.wait_recv()
        total[...] += got[count + i].astype(f32)
    out_ref[...] = total[...].astype(out_ref.dtype)
    for copy in crossed + sent:
        copy.wait_send()
    for d in range(1, pairs):
        for copy in states[d - 1]:
            pl.when(pair + d < pairs)(copy.wait_send)

    @pl.when(pair < pairs - 1)
    def _():
        for copy in edges:
            copy.wait_send()

    ring_sent = [c for some in (rings, out_rings) for copies in some.values() for c in copies]
    for copy in swap + spread + passed + ring_sent:
        copy.wait_send()


def mixed_rows(rows_in, weights, gate_weight, bias, taps, gain, own_group, pool_gain):
    pairs, n_tp = lax.axis_size("sp") // 2, lax.axis_size("tp")
    tall = n_tp // 2
    f32, bf16 = jnp.float32, jnp.bfloat16
    vmem = pl.BlockSpec(memory_space=pltpu.VMEM)
    dma = pltpu.SemaphoreType.DMA
    slots, steps = 4 * tall - 1, pairs // 2
    head, group = gain.shape[1], pool_gain.shape[1]
    tokens = rows_in.shape[0] - 16
    span, features, height = 2 * tokens, rows_in.shape[1] * n_tp, tokens // n_tp
    depth, projected = weights[0].shape[0], 4 * head + group
    out_columns = weights[5].shape[1]
    width = out_columns * 2 * pairs
    scratch = [
        ((2, rows_in.shape[0], features), bf16),
        ((2 * pairs, depth, projected), bf16),
        ((2 * pairs, head + group, out_columns), bf16),
        ((span, features), bf16),
        ((span, 128), f32),
        ((span, 128), f32),
        ((span, projected), f32),
        ((span, projected), bf16),
        ((head + group, width), bf16),
        ((16, 2 * head), bf16),
        ((16, group), bf16),
        ((span + 16, 2 * head), f32),
        ((span + 16, group), f32),
        ((span, head), bf16),
        ((span, head), bf16),
        ((span, head), f32),
        ((span, 128), f32),
        ((span, head + group), bf16),
        ((head, head), bf16),
        ((8, head), f32),
        ((pairs - 1, head, head), bf16),
        ((pairs - 1, 8, head), f32),
        ((slots, height, width), bf16),
        ((slots, height, width), bf16),
        ((height, width), f32),
    ]
    return pl.pallas_call(
        functools.partial(mixer_kernel, pairs, tall, tokens, head, group),
        out_shape=jax.ShapeDtypeStruct((height, width), bf16),
        in_specs=[vmem] + [pl.BlockSpec(memory_space=pl.ANY)] * 7 + [vmem] * 6,
        out_specs=vmem,
        scratch_shapes=[pltpu.VMEM(shape, kind) for shape, kind in scratch] + [
            dma((8,)),
            dma((2 * tall,)), dma((2 * tall,)),
            dma((2 * tall,)), dma((2 * tall,)),
            dma((7,)), dma((7,)),
            dma((steps * 4, 2)), dma((steps * 4, 2)),
            dma((4,)), dma((pairs - 1, 2)), dma((pairs - 1, 2)),
            dma((2 * tall,)), dma((2 * tall,)), dma((2 * tall,)), dma((2 * tall,)),
        ],
        compiler_params=pltpu.CompilerParams(
            collective_id=0, has_side_effects=True, vmem_limit_bytes=63 * 2**20
        ),
    )(rows_in, *weights, gate_weight, bias, taps, gain, own_group, pool_gain)


def local(
    inputs,
    norm_gain,
    query_weight,
    key_weight,
    value_weight,
    outgate_weight,
    inputgate_weight,
    forget_weight,
    forget_bias,
    conv_query,
    conv_key,
    cell_gain,
    pool_weight,
    group_weight,
    pool_gain,
    cell_out_weight,
    pool_out_weight,
):
    f32, bf16 = jnp.float32, jnp.bfloat16
    sp_index, tp_index = lax.axis_index("sp"), lax.axis_index("tp")
    n_sp = lax.axis_size("sp")
    pairs = n_sp // 2
    pair, half = sp_index // 2, sp_index % 2
    tokens_here = inputs.shape[0]
    span = 2 * tokens_here
    local_heads = forget_bias.shape[0]
    head = query_weight.shape[1] // 2
    group = pool_weight.shape[1] // 2

    gain_rows = jnp.broadcast_to(norm_gain[None, :], (16, norm_gain.shape[0]))
    rows_in = jnp.concatenate([inputs, gain_rows], axis=0)
    head_index = tp_index * local_heads + half
    gate_cols = jnp.concatenate(
        [
            lax.dynamic_slice_in_dim(inputgate_weight, head_index, 1, 1),
            lax.dynamic_slice_in_dim(forget_weight, head_index, 1, 1),
        ],
        axis=1,
    )
    gate_weight = jnp.pad(gate_cols, ((0, 0), (0, 126)))
    sequence_log = math.log(tokens_here * n_sp)
    bias = jnp.broadcast_to(forget_bias[half] + sequence_log, (1, 128))

    def own(array, axis, width):
        return lax.dynamic_slice_in_dim(array, half * width, width, axis)

    taps = jnp.concatenate([own(conv_query, 1, head), own(conv_key, 1, head)], axis=1)
    own_group = lax.dynamic_index_in_dim(group_weight, half, 0, keepdims=False)
    return mixed_rows(
        rows_in,
        (
            query_weight,
            key_weight,
            value_weight,
            outgate_weight,
            pool_weight,
            cell_out_weight,
            pool_out_weight,
        ),
        gate_weight,
        bias,
        taps,
        own(cell_gain, 0, head)[None],
        own_group,
        own(pool_gain, 0, group)[None],
    )


def solution(mesh):
    in_specs = (
        P("sp", "tp"),
        P("tp"),
        P("sp", "tp"),
        P("sp", "tp"),
        P("sp", "tp"),
        P("sp", "tp"),
        P(),
        P(),
        P("tp"),
        P(None, "tp"),
        P(None, "tp"),
        P("tp"),
        P("sp", "tp"),
        P("tp", None, None),
        P("tp"),
        P("tp", "sp"),
        P("tp", "sp"),
    )
    out_specs = P(("sp", "tp"), None)
    return jax.shard_map(local, mesh=mesh, in_specs=in_specs, out_specs=out_specs, check_vma=False)
```
